768 devices in a mesh: sp: 48 (over z, x), tp: 16 (over y, core).
Axes of the slice: x: 4, y: 8, z: 12, core: 2. Of those that a mesh axis runs over, the one named last changes fastest.
Arguments:
- grid_in: bfloat16 [6144, 2048], P('sp', 'tp'), may hold values from -6 to 6
- documents: int32 [6144], P('sp'), may hold values from 0 to 23, never falling along the last dimension, each value on 1 to 512 neighbouring positions
- pre_gain: float32 [2, 2048], replicated, may hold values from 0.1 to 1.9
- query_weight: bfloat16 [2, 2048, 2048], P(None, None, 'tp'), may hold values from -1 to 1
- key_weight: bfloat16 [2, 2048, 2048], P(None, None, 'tp'), may hold values from -4 to 4
- value_weight: bfloat16 [2, 2048, 2048], P(None, None, 'tp'), may hold values from -0.125 to 0.125
- offset_bias: float32 [2, 32, 15, 31], P(None, 'tp'), may hold values from -5 to 5
- out_weight: bfloat16 [2, 2048, 2048], P(None, None, 'tp'), may hold values from -3 to 3
- post_gain: float32 [2, 2048], P(None, 'tp'), may hold values from 0.1 to 1.9
Outputs:
- grid_out: bfloat16 [6144, 2048], P('sp', 'tp')
The draws below stay inside these ranges and needn't reach their ends.
Inputs may be any that keep to these rules, and one draw needn't show every extreme that they name: `documents`: each position's document number; numbers never fall along the token order, and each document covers 1 to 512 positions.
All inputs are finite; a program needn't handle non-finite values.
Results may differ from the reference program's by a relative error of at most 0.0095.
Values may be sent and summed in bfloat16 or wider, within the bound.
No kernel may reach another device: no remote copies, remote signals or barrier semaphores. Data moves between devices by JAX's collectives and lax.ppermute only.
A program may use at most 64 MiB of HBM per device.

```python
import math
import jax
import jax.numpy as jnp
import numpy as np
from jax import lax

D = 2048
HEADS = 32
HEAD_DIM = 64
WIN_ROWS = 8
WIN_COLS = 16
GRID_W = 32
LAYERS = 2
TOKENS = 6144
DOCS = 24
DOC_MOST = 512


def paired_weights(key):
    sigma = D ** (-0.5)
    base_draw = jax.random.normal(jax.random.fold_in(key, 101), (LAYERS, D, D), jnp.float32) * sigma
    other_draw = jax.random.normal(jax.random.fold_in(key, 102), (LAYERS, D, D), jnp.float32) * sigma
    return (jnp.clip(base_draw, -6.0 * sigma, 6.0 * sigma), jnp.clip(other_draw, -6.0 * sigma, 6.0 * sigma))


def draw_query_weight(key, part):
    base_draw, other_draw = paired_weights(key)
    return base_draw.astype(jnp.bfloat16)


def draw_key_weight(key, part):
    base_draw, other_draw = paired_weights(key)
    result = other_draw
    return result.astype(jnp.bfloat16)


def draw_out_weight(key, part):
    sigma = D ** (-0.5)
    drawn = jnp.clip(jax.random.normal(jax.random.fold_in(key, 104), (LAYERS, D, D), jnp.float32), -6.0, 6.0) * sigma
    rising = 10.0 ** (jnp.arange(D, dtype=jnp.float32) / D)
    rough = jnp.exp(jax.random.uniform(jax.random.fold_in(key, 105), (LAYERS, 1, D), jnp.float32, -0.4, 0.4))
    return jnp.clip(drawn * rising[None, None, :] * rough, -3.0, 3.0).astype(jnp.bfloat16)


def level_of(own_key, dims, split, smallest, high):
    def one(position, shards_of):
        heights = jax.random.uniform(jax.random.fold_in(jax.random.fold_in(own_key, 6), position), (shards_of,), jnp.float32, smallest / len(split), high / len(split))
        return jnp.repeat(jnp.exp(heights), dims[position] // shards_of).reshape((-1,) + (1,) * (len(dims) - position - 1))

    level = one(*split[0])
    for cut in split[1:]:
        level = level * one(*cut)
    return level


def length_profile(count, total, reach, lean):
    loads = [(1 << 20) // math.isqrt(rank ** lean) + 1 for rank in range(2, count + 1)]
    rest, counts = total - reach - (count - 1), [1] * (count - 1)
    while rest > 0:
        candidates = [i for i in range(count - 1) if counts[i] < reach]
        whole, budget = sum([loads[i] for i in candidates]), rest
        for i in candidates:
            extra = min(reach - counts[i], max(1, budget * loads[i] // whole), rest)
            counts[i] = counts[i] + extra
            rest = rest - extra
    return np.array([reach] + counts)


def uneven_parts(rng, count, total, bound, slope):
    if count == 2:
        one = jax.random.randint(rng, (), max(1, total - bound), min(bound, total - 1) + 1)
        return jnp.stack([one, total - one])
    lengths = jnp.asarray(length_profile(count, total, bound, slope), jnp.int32)
    pairs = (count - 1) // 2
    source_of, taker = lengths[1:1 + 2 * pairs:2], lengths[2:2 + 2 * pairs:2]
    slack = jnp.minimum(source_of - 1, bound - taker)
    passed = jax.random.randint(jax.random.fold_in(rng, 1), (pairs,), 0, 1 << 20) % (slack + 1)
    lengths = lengths.at[1:1 + 2 * pairs:2].set(source_of - passed).at[2:2 + 2 * pairs:2].set(taker + passed)
    return lengths[jax.random.permutation(jax.random.fold_in(rng, 2), count)]


def noise(own_key, dims, spread, reach, shards=(), kind=jnp.bfloat16):
    factor_of = level_of(own_key, dims, shards, -0.22, 0.18) if shards else 1.0
    values = jax.random.normal(own_key, dims, jnp.float32) * spread * factor_of
    return jnp.minimum(jnp.maximum(values, -reach), reach).astype(kind)


def setup_inputs(seed: int = 0) -> dict:
    arg_keys = jax.random.split(jax.random.key(seed), 10)
    grid_in = noise(arg_keys[0], (TOKENS, D), 1.0, 6.0, ((0, 48), (1, 16)))
    documents = jnp.searchsorted(jnp.cumsum(uneven_parts(arg_keys[1], DOCS, TOKENS, DOC_MOST, 0)), jnp.arange(TOKENS), side="right").astype(jnp.int32)
    pre_gain = jnp.clip(1.0 + 0.18 * jax.random.normal(arg_keys[2], (LAYERS, D), jnp.float32), 0.1, 1.9)
    query_weight = draw_query_weight(jax.random.fold_in(arg_keys[9], 71), 0)
    key_weight = draw_key_weight(jax.random.fold_in(arg_keys[9], 71), 0)
    value_weight = noise(arg_keys[5], (LAYERS, D, D), D ** -0.5, 0.125, ((2, 16),))
    offset_bias = noise(arg_keys[6], (LAYERS, HEADS, 2 * WIN_ROWS - 1, 2 * WIN_COLS - 1), 1.0, 5.0, ((1, 16),), jnp.float32)
    out_weight = draw_out_weight(jax.random.fold_in(arg_keys[9], 71), 0)
    post_gain = jnp.clip(1.0 + 0.18 * jax.random.normal(arg_keys[8], (LAYERS, D), jnp.float32), 0.1, 1.9)
    return {"grid_in": grid_in, "documents": documents, "pre_gain": pre_gain, "query_weight": query_weight, "key_weight": key_weight, "value_weight": value_weight, "offset_bias": offset_bias, "out_weight": out_weight, "post_gain": post_gain}


epsilon = 1e-06

def reference(grid_in, documents, pre_gain, query_weight, key_weight, value_weight, offset_bias, out_weight, post_gain):
    tokens_all, model_width = grid_in.shape
    grid_rows = tokens_all // GRID_W
    rim_rows = WIN_ROWS // 2
    score_scale = HEAD_DIM ** (-0.5)
    columns = jnp.arange(GRID_W, dtype=jnp.int32)
    col_start = jnp.clip(columns - WIN_COLS // 2, 0, GRID_W - WIN_COLS)
    col_allowed = (columns[None, :] >= col_start[:, None]) & (columns[None, :] < col_start[:, None] + WIN_COLS)
    col_offset = jnp.clip(columns[None, :] - columns[:, None] + WIN_COLS - 1, 0, 2 * WIN_COLS - 2)
    doc_grid = documents.reshape(grid_rows, GRID_W)
    stream = grid_in
    for layer_index in range(LAYERS):
        widened = stream.astype(jnp.float32)
        scaler = lax.rsqrt(lax.optimization_barrier(jnp.mean(widened * widened, axis=1, keepdims=True)) + epsilon)
        scaled = (widened * pre_gain[layer_index][None, :]).astype(jnp.bfloat16)
        query_rows = (jnp.dot(scaled, query_weight[layer_index], preferred_element_type=jnp.float32) * scaler).astype(jnp.bfloat16)
        key_rows = (jnp.dot(scaled, key_weight[layer_index], preferred_element_type=jnp.float32) * scaler).astype(jnp.bfloat16)
        value_rows = (jnp.dot(scaled, value_weight[layer_index], preferred_element_type=jnp.float32) * scaler).astype(jnp.bfloat16)
        query_grid = query_rows.reshape(grid_rows, GRID_W, HEADS, HEAD_DIM)
        key_grid = key_rows.reshape(grid_rows, GRID_W, HEADS, HEAD_DIM)
        value_grid = value_rows.reshape(grid_rows, GRID_W, HEADS, HEAD_DIM)
        col_bias = offset_bias[layer_index][:, :, col_offset]

        def one_row(row_at):
            slab_start = jnp.clip(row_at - rim_rows, 0, grid_rows - WIN_ROWS).astype(jnp.int32)
            key_slab = lax.dynamic_slice_in_dim(key_grid, slab_start, WIN_ROWS, 0).astype(jnp.float32)
            value_slab = lax.dynamic_slice_in_dim(value_grid, slab_start, WIN_ROWS, 0).astype(jnp.float32)
            doc_slab = lax.dynamic_slice_in_dim(doc_grid, slab_start, WIN_ROWS, 0)
            query_row = lax.dynamic_index_in_dim(query_grid, row_at, 0, keepdims=False).astype(jnp.float32)
            own_docs = lax.dynamic_index_in_dim(doc_grid, row_at, 0, keepdims=False)
            scores = jnp.einsum('chd,jkhd->hcjk', query_row, key_slab) * score_scale
            bias_rows = lax.dynamic_slice_in_dim(col_bias, (slab_start - row_at + WIN_ROWS - 1).astype(jnp.int32), WIN_ROWS, 1)
            scores = scores + jnp.transpose(bias_rows, (0, 2, 1, 3))
            allowed = (doc_slab[None, :, :] == own_docs[:, None, None]) & col_allowed[:, None, :]
            scores = jnp.where(allowed[None], scores, -jnp.inf)
            row_peak = lax.optimization_barrier(jnp.max(scores, axis=(2, 3), keepdims=True))
            lifted = jnp.exp(scores - row_peak)
            weights = (lifted / lax.optimization_barrier(jnp.sum(lifted, axis=(2, 3), keepdims=True))).astype(jnp.bfloat16)
            return jnp.einsum('hcjk,jkhd->chd', weights.astype(jnp.float32), value_slab).astype(jnp.bfloat16)
        attended = lax.map(one_row, jnp.arange(grid_rows, dtype=jnp.int32)).reshape(tokens_all, model_width)
        branch = jnp.dot(attended, out_weight[layer_index], preferred_element_type=jnp.float32)
        branch_scale = lax.rsqrt(lax.optimization_barrier(jnp.mean(branch * branch, axis=1, keepdims=True)) + epsilon)
        stream = (widened + branch * branch_scale * post_gain[layer_index][None, :]).astype(jnp.bfloat16)
    return stream
```

```python
import functools

import jax
import jax.numpy as jnp
from jax import lax
from jax.experimental import pallas as pl
from jax.experimental.pallas import tpu as pltpu
from jax.sharding import PartitionSpec as P

HEAD_DIM = 64
WIN_ROWS = 8
WIN_COLS = 16
GRID_W = 32
LAYERS = 2
EPSILON = 1e-06
RIM = WIN_ROWS // 2
BIAS_ROWS = 2 * WIN_ROWS
LOWEST = -1e30

VMEM = pl.BlockSpec(memory_space=pltpu.VMEM)
SMEM = pl.BlockSpec(memory_space=pltpu.SMEM)


def call(body, outs, specs, name):
    return pl.pallas_call(
        body,
        out_shape=outs,
        in_specs=specs,
        out_specs=jax.tree.map(lambda _: VMEM, outs),
        name=name,
    )


def struct(shape, dtype):
    return jax.ShapeDtypeStruct(shape, dtype)


def joined(ref, rows):
    return jnp.concatenate([ref[i, :rows] for i in range(ref.shape[0])], axis=1)


def as_column(row, size):
    return jnp.transpose(jnp.broadcast_to(row, (size, size)))


def heads_from(wide, gain, weights, q_ref, kv_ref):
    tokens, model_width = wide.shape
    cols = weights[0].shape[1]
    scaler = lax.rsqrt(jnp.sum(wide * wide, axis=1, keepdims=True) / model_width + EPSILON)
    scaled = (wide * gain).astype(jnp.bfloat16)
    query, key, value = (
        (jnp.dot(scaled, w, preferred_element_type=jnp.float32) * scaler).astype(jnp.bfloat16)
        for w in weights
    )
    q_ref[...] = query
    kv_ref[:tokens, :cols] = key
    kv_ref[:tokens, cols:] = value


def first_heads(x_ref, gain_ref, docs_ref, wq_ref, wk_ref, wv_ref, q_ref, kv_ref):
    tokens = x_ref.shape[1]
    wide = joined(x_ref, tokens).astype(jnp.float32)
    heads_from(wide, gain_ref[0:1], (wq_ref[0], wk_ref[0], wv_ref[0]), q_ref, kv_ref)
    pad = kv_ref.shape[0] - tokens
    row = docs_ref[...].astype(jnp.float32)
    row = jnp.concatenate([row] * (kv_ref.shape[1] // tokens), axis=1)
    kv_ref[tokens:] = jnp.broadcast_to(row, (pad, kv_ref.shape[1])).astype(jnp.bfloat16)


def next_heads(at_ref, x_ref, b_ref, gain_ref, own_gain_ref, wq_ref, wk_ref, wv_ref, q_ref, kv_ref, own_ref):
    tokens = x_ref.shape[1]
    count = x_ref.shape[0]
    branch = joined(b_ref, tokens).astype(jnp.float32)
    scale = lax.rsqrt(jnp.sum(branch * branch, axis=1, keepdims=True) / branch.shape[1] + EPSILON)
    parts = jnp.concatenate([b_ref[i, tokens:] for i in range(count)], axis=1).astype(jnp.float32)
    post = parts[0:1] + parts[1:2] + parts[2:3]
    stream = joined(x_ref, tokens).astype(jnp.float32)
    stream = (stream + branch * scale * post).astype(jnp.bfloat16)
    heads_from(
        stream.astype(jnp.float32), gain_ref[1:2], (wq_ref[1], wk_ref[1], wv_ref[1]), q_ref, kv_ref
    )
    at = at_ref[0]
    own = x_ref[at].astype(jnp.float32)
    own_branch = b_ref[at][:tokens].astype(jnp.float32)
    own_ref[...] = (own + own_branch * scale * own_gain_ref[0:1]).astype(jnp.bfloat16)


def attend(layer, last_row, at_ref, q_ref, own_ref, low_ref, high_ref, dl_ref, do_ref, dh_ref, bias_ref, out_ref):
    tokens, cols = q_ref.shape
    rows = tokens // GRID_W
    keys = 3 * tokens
    first_row = at_ref[1] * rows
    blocks = (low_ref, own_ref, high_ref)
    key = jnp.concatenate([b[:tokens, :cols] for b in blocks], axis=0)
    value = jnp.concatenate([b[:tokens, cols:] for b in blocks], axis=0)
    key_docs = jnp.concatenate([d[:1, :tokens].astype(jnp.float32) for d in (dl_ref, do_ref, dh_ref)], axis=1)
    query_docs = as_column(do_ref[:1, :tokens].astype(jnp.float32), tokens)
    query_docs = jnp.concatenate([query_docs] * 3, axis=1)
    token = lax.broadcasted_iota(jnp.int32, (tokens, keys), 0)
    other = lax.broadcasted_iota(jnp.int32, (tokens, keys), 1)
    row, col = first_row + token // GRID_W, token % GRID_W
    key_row, key_col = first_row - rows + other // GRID_W, other % GRID_W
    row_start = jnp.clip(row - RIM, 0, last_row - WIN_ROWS)
    col_start = jnp.clip(col - WIN_COLS // 2, 0, GRID_W - WIN_COLS)
    allowed = (
        (key_row >= row_start)
        & (key_row < row_start + WIN_ROWS)
        & (key_col >= col_start)
        & (key_col < col_start + WIN_COLS)
        & (key_docs == query_docs)
    )
    query = q_ref[...]
    lane = lax.broadcasted_iota(jnp.int32, (tokens, cols), 1)
    result = jnp.zeros((tokens, cols), jnp.float32)
    for head in range(cols // HEAD_DIM):
        mine = (lane >= head * HEAD_DIM) & (lane < (head + 1) * HEAD_DIM)
        flat = jnp.broadcast_to(bias_ref[layer, head : head + 1], (GRID_W, bias_ref.shape[2]))
        width = flat.shape[1]
        bias = jnp.concatenate(
            [
                pltpu.roll(
                    flat,
                    (-(WIN_COLS - 1) - (WIN_ROWS - 1 - rows - r) * GRID_W) % width,
                    1,
                    stride=1,
                    stride_axis=0,
                )[:, :keys]
                for r in range(rows)
            ],
            axis=0,
        )
        scores = lax.dot_general(
            jnp.where(mine, query, jnp.zeros_like(query)),
            key,
            (((1,), (1,)), ((), ())),
            preferred_element_type=jnp.float32,
        )
        scores = jnp.where(allowed, scores * HEAD_DIM ** (-0.5) + bias, LOWEST)
        lifted = jnp.exp(scores - jnp.max(scores, axis=1, keepdims=True))
        weights = (lifted / jnp.sum(lifted, axis=1, keepdims=True)).astype(jnp.bfloat16)
        summed = jnp.dot(weights, value, preferred_element_type=jnp.float32)
        result = jnp.where(mine, summed, result)
    out_ref[...] = result.astype(jnp.bfloat16)


def first_out(a_ref, w_ref, post_ref, out_ref):
    tokens = a_ref.shape[1]
    branch = jnp.dot(joined(a_ref, tokens), w_ref[0], preferred_element_type=jnp.float32)
    out_ref[:tokens] = branch.astype(jnp.bfloat16)
    post = post_ref[0:1]
    high = post.astype(jnp.bfloat16)
    rest = post - high.astype(jnp.float32)
    middle = rest.astype(jnp.bfloat16)
    low = (rest - middle.astype(jnp.float32)).astype(jnp.bfloat16)
    pad = out_ref.shape[0] - tokens
    place = lax.broadcasted_iota(jnp.int32, (pad, post.shape[1]), 0)
    rows = jnp.where(
        place == 0,
        high.astype(jnp.float32),
        jnp.where(place == 1, middle.astype(jnp.float32), low.astype(jnp.float32)),
    )
    out_ref[tokens:] = rows.astype(jnp.bfloat16)


def last_out(a_ref, w_ref, branch_ref, squares_ref):
    tokens = a_ref.shape[1]
    branch = jnp.dot(joined(a_ref, tokens), w_ref[1], preferred_element_type=jnp.float32)
    branch_ref[...] = branch
    squares = jnp.sum(jnp.transpose(branch * branch), axis=0, keepdims=True)
    squares_ref[...] = jnp.broadcast_to(squares[None], squares_ref.shape)


def finish(model_width, squares_ref, branch_ref, own_ref, post_ref, out_ref):
    tokens = branch_ref.shape[0]
    total = jnp.sum(squares_ref[...], axis=0)
    scale = as_column(lax.rsqrt(total / model_width + EPSILON), tokens)
    out_ref[...] = (
        own_ref[...].astype(jnp.float32) + branch_ref[...] * scale * post_ref[1:2]
    ).astype(jnp.bfloat16)


def neighbours(block):
    count = lax.axis_size("sp")
    forward = [(i, i + 1) for i in range(count - 1)]
    backward = [(i + 1, i) for i in range(count - 1)]
    return lax.ppermute(block, "sp", forward), lax.ppermute(block, "sp", backward)


def shards(
    grid_in,
    documents,
    pre_gain,
    query_weight,
    key_weight,
    value_weight,
    offset_bias,
    out_weight,
    post_gain,
):
    tokens, feat = grid_in.shape
    model_width = pre_gain.shape[1]
    cols = query_weight.shape[2]
    heads = offset_bias.shape[1]
    bf16, f32 = jnp.bfloat16, jnp.float32
    members = lax.axis_size("tp")
    all_rows = tokens // GRID_W * lax.axis_size("sp")
    pad = 16
    at = jnp.stack([lax.axis_index("tp"), lax.axis_index("sp")]).astype(jnp.int32)
    docs = documents.reshape(1, tokens)
    bias = jnp.pad(
        offset_bias, ((0, 0), (0, 0), (0, BIAS_ROWS - 2 * WIN_ROWS + 1), (0, GRID_W - 2 * WIN_COLS + 1))
    ).reshape(LAYERS, heads, BIAS_ROWS * GRID_W)

    stream = lax.all_gather(grid_in, "tp", axis=0)
    query, kv = call(
        first_heads,
        (struct((tokens, cols), bf16), struct((tokens + pad, 2 * cols), bf16)),
        [VMEM] * 6,
        "first_heads",
    )(stream, pre_gain, docs, query_weight, key_weight, value_weight)
    low, high = neighbours(kv)
    doc_rows = (low[tokens:], kv[tokens:], high[tokens:])

    def attention(layer, query, kv, low, high):
        return call(
            functools.partial(attend, layer, all_rows),
            struct((tokens, cols), bf16),
            [SMEM] + [VMEM] * 8,
            "attend%d" % layer,
        )(at, query, kv, low, high, *doc_rows, bias)

    attended = lax.all_gather(attention(0, query, kv, low, high), "tp", axis=0)
    branch = call(first_out, struct((tokens + pad, feat), bf16), [VMEM] * 3, "first_out")(
        attended, out_weight, post_gain
    )
    branch = lax.all_gather(branch, "tp", axis=0)
    query, kv, own = call(
        next_heads,
        (
            struct((tokens, cols), bf16),
            struct((tokens, 2 * cols), bf16),
            struct((tokens, feat), bf16),
        ),
        [SMEM] + [VMEM] * 7,
        "next_heads",
    )(at, stream, branch, pre_gain, post_gain, query_weight, key_weight, value_weight)
    low, high = neighbours(kv)
    attended = lax.all_gather(attention(1, query, kv, low, high), "tp", axis=0)
    branch, squares = call(
        last_out,
        (struct((tokens, feat), f32), struct((members, 1, tokens), f32)),
        [VMEM] * 2,
        "last_out",
    )(attended, out_weight)
    squares = lax.all_to_all(squares, "tp", 0, 0, tiled=True)
    return call(
        functools.partial(finish, model_width), struct((tokens, feat), bf16), [VMEM] * 4, "finish"
    )(squares, branch, own, post_gain)


def solution(mesh):
    return jax.shard_map(
        shards,
        mesh=mesh,
        in_specs=(
            P("sp", "tp"),
            P("sp"),
            P(),
            P(None, None, "tp"),
            P(None, None, "tp"),
            P(None, None, "tp"),
            P(None, "tp", None, None),
            P(None, None, "tp"),
            P(None, "tp"),
        ),
        out_specs=P("sp", "tp"),
        check_vma=False,
    )
```

```python
import functools

import jax
import jax.numpy as jnp
from jax import lax
from jax.experimental import pallas as pl
from jax.experimental.pallas import tpu as pltpu
from jax.sharding import PartitionSpec as P

HEAD_DIM = 64
WIN_ROWS = 8
WIN_COLS = 16
GRID_W = 32
LAYERS = 2
EPSILON = 1e-06
RIM = WIN_ROWS // 2
BIAS_ROWS = 2 * WIN_ROWS
LOWEST = -1e30

VMEM = pl.BlockSpec(memory_space=pltpu.VMEM)
SMEM = pl.BlockSpec(memory_space=pltpu.SMEM)


def call(body, outs, specs, name):
    kernel = pl.pallas_call(
        body,
        out_shape=outs,
        in_specs=specs,
        out_specs=jax.tree.map(lambda _: VMEM, outs),
        name=name,
    )

    def run(*args):
        return kernel(
            *(
                pltpu.with_memory_space_constraint(arg, pltpu.VMEM) if spec is VMEM else arg
                for arg, spec in zip(args, specs, strict=True)
            )
        )

    return run


def struct(shape, dtype):
    return pltpu.VMEM(shape, dtype)


def of(array, layer):
    return lax.slice_in_dim(array, layer, layer + 1, axis=0)


def joined(ref, rows):
    return jnp.concatenate([ref[i, :rows] for i in range(ref.shape[0])], axis=1)


def as_column(row, size):
    return jnp.transpose(jnp.broadcast_to(row, (size, size)))


def heads_from(wide, gain, weights, q_ref, kv_ref):
    tokens, model_width = wide.shape
    cols = weights[0].shape[1]
    scaler = lax.rsqrt(jnp.sum(wide * wide, axis=1, keepdims=True) / model_width + EPSILON)
    scaled = (wide * gain).astype(jnp.bfloat16)
    query, key, value = (
        (jnp.dot(scaled, w, preferred_element_type=jnp.float32) * scaler).astype(jnp.bfloat16)
        for w in weights
    )
    q_ref[...] = query
    kv_ref[:tokens, :cols] = key
    kv_ref[:tokens, cols:] = value


def first_heads(x_ref, gain_ref, docs_ref, wq_ref, wk_ref, wv_ref, q_ref, kv_ref):
    tokens = x_ref.shape[1]
    wide = joined(x_ref, tokens).astype(jnp.float32)
    heads_from(wide, gain_ref[0:1], (wq_ref[0], wk_ref[0], wv_ref[0]), q_ref, kv_ref)
    pad = kv_ref.shape[0] - tokens
    row = docs_ref[...].astype(jnp.float32)
    row = jnp.concatenate([row] * (kv_ref.shape[1] // tokens), axis=1)
    kv_ref[tokens:] = jnp.broadcast_to(row, (pad, kv_ref.shape[1])).astype(jnp.bfloat16)


def next_heads(at_ref, x_ref, b_ref, gain_ref, own_gain_ref, wq_ref, wk_ref, wv_ref, q_ref, kv_ref, own_ref):
    tokens = x_ref.shape[1]
    count = x_ref.shape[0]
    branch = joined(b_ref, tokens).astype(jnp.float32)
    scale = lax.rsqrt(jnp.sum(branch * branch, axis=1, keepdims=True) / branch.shape[1] + EPSILON)
    parts = jnp.concatenate([b_ref[i, tokens:] for i in range(count)], axis=1).astype(jnp.float32)
    post = parts[0:1] + parts[1:2] + parts[2:3]
    stream = joined(x_ref, tokens).astype(jnp.float32)
    stream = (stream + branch * scale * post).astype(jnp.bfloat16)
    heads_from(
        stream.astype(jnp.float32), gain_ref[0:1], (wq_ref[0], wk_ref[0], wv_ref[0]), q_ref, kv_ref
    )
    at = at_ref[0]
    own = x_ref[at].astype(jnp.float32)
    own_branch = b_ref[at][:tokens].astype(jnp.float32)
    own_ref[...] = (own + own_branch * scale * own_gain_ref[0:1]).astype(jnp.bfloat16)


def attend(layer, last_row, at_ref, q_ref, own_ref, low_ref, high_ref, dl_ref, do_ref, dh_ref, bias_ref, out_ref):
    tokens, cols = q_ref.shape
    rows = tokens // GRID_W
    keys = 3 * tokens
    first_row = at_ref[1] * rows
    blocks = (low_ref, own_ref, high_ref)
    key = jnp.concatenate([b[:tokens, :cols] for b in blocks], axis=0)
    value = jnp.concatenate([b[:tokens, cols:] for b in blocks], axis=0)
    key_docs = jnp.concatenate([d[:1, :tokens].astype(jnp.float32) for d in (dl_ref, do_ref, dh_ref)], axis=1)
    query_docs = as_column(do_ref[:1, :tokens].astype(jnp.float32), tokens)
    query_docs = jnp.concatenate([query_docs] * 3, axis=1)
    token = lax.broadcasted_iota(jnp.int32, (tokens, keys), 0)
    other = lax.broadcasted_iota(jnp.int32, (tokens, keys), 1)
    row, col = first_row + token // GRID_W, token % GRID_W
    key_row, key_col = first_row - rows + other // GRID_W, other % GRID_W
    row_start = jnp.clip(row - RIM, 0, last_row - WIN_ROWS)
    col_start = jnp.clip(col - WIN_COLS // 2, 0, GRID_W - WIN_COLS)
    allowed = (
        (key_row >= row_start)
        & (key_row < row_start + WIN_ROWS)
        & (key_col >= col_start)
        & (key_col < col_start + WIN_COLS)
        & (key_docs == query_docs)
    )
    query = q_ref[...]
    lane = lax.broadcasted_iota(jnp.int32, (tokens, cols), 1)
    result = jnp.zeros((tokens, cols), jnp.float32)
    for head in range(cols // HEAD_DIM):
        mine = (lane >= head * HEAD_DIM) & (lane < (head + 1) * HEAD_DIM)
        flat = jnp.broadcast_to(bias_ref[layer, head : head + 1], (GRID_W, bias_ref.shape[2]))
        width = flat.shape[1]
        bias = jnp.concatenate(
            [
                pltpu.roll(
                    flat,
                    (-(WIN_COLS - 1) - (WIN_ROWS - 1 - rows - r) * GRID_W) % width,
                    1,
                    stride=1,
                    stride_axis=0,
                )[:, :keys]
                for r in range(rows)
            ],
            axis=0,
        )
        scores = lax.dot_general(
            jnp.where(mine, query, jnp.zeros_like(query)),
            key,
            (((1,), (1,)), ((), ())),
            preferred_element_type=jnp.float32,
        )
        scores = jnp.where(allowed, scores * HEAD_DIM ** (-0.5) + bias, LOWEST)
        lifted = jnp.exp(scores - jnp.max(scores, axis=1, keepdims=True))
        weights = (lifted / jnp.sum(lifted, axis=1, keepdims=True)).astype(jnp.bfloat16)
        summed = jnp.dot(weights, value, preferred_element_type=jnp.float32)
        result = jnp.where(mine, summed, result)
    out_ref[...] = result.astype(jnp.bfloat16)


def first_out(a_ref, w_ref, post_ref, out_ref):
    tokens = a_ref.shape[1]
    branch = jnp.dot(joined(a_ref, tokens), w_ref[0], preferred_element_type=jnp.float32)
    out_ref[:tokens] = branch.astype(jnp.bfloat16)
    post = post_ref[0:1]
    high = post.astype(jnp.bfloat16)
    rest = post - high.astype(jnp.float32)
    middle = rest.astype(jnp.bfloat16)
    low = (rest - middle.astype(jnp.float32)).astype(jnp.bfloat16)
    pad = out_ref.shape[0] - tokens
    place = lax.broadcasted_iota(jnp.int32, (pad, post.shape[1]), 0)
    rows = jnp.where(
        place == 0,
        high.astype(jnp.float32),
        jnp.where(place == 1, middle.astype(jnp.float32), low.astype(jnp.float32)),
    )
    out_ref[tokens:] = rows.astype(jnp.bfloat16)


def last_out(a_ref, w_ref, branch_ref, squares_ref):
    tokens = a_ref.shape[1]
    branch = jnp.dot(joined(a_ref, tokens), w_ref[0], preferred_element_type=jnp.float32)
    branch_ref[...] = branch
    squares = jnp.sum(jnp.transpose(branch * branch), axis=0, keepdims=True)
    squares_ref[...] = jnp.broadcast_to(squares[None], squares_ref.shape)


def finish(model_width, squares_ref, branch_ref, own_ref, post_ref, out_ref):
    tokens = branch_ref.shape[0]
    total = jnp.sum(squares_ref[...], axis=0)
    scale = as_column(lax.rsqrt(total / model_width + EPSILON), tokens)
    out_ref[...] = (
        own_ref[...].astype(jnp.float32) + branch_ref[...] * scale * post_ref[0:1]
    ).astype(jnp.bfloat16)


def neighbours(block):
    count = lax.axis_size("sp")
    forward = [(i, i + 1) for i in range(count - 1)]
    backward = [(i + 1, i) for i in range(count - 1)]
    return lax.ppermute(block, "sp", forward), lax.ppermute(block, "sp", backward)


def shards(
    grid_in,
    documents,
    pre_gain,
    query_weight,
    key_weight,
    value_weight,
    offset_bias,
    out_weight,
    post_gain,
):
    tokens, feat = grid_in.shape
    model_width = pre_gain.shape[1]
    cols = query_weight.shape[2]
    heads = offset_bias.shape[1]
    bf16, f32 = jnp.bfloat16, jnp.float32
    members = lax.axis_size("tp")
    all_rows = tokens // GRID_W * lax.axis_size("sp")
    pad = 16
    at = jnp.stack([lax.axis_index("tp"), lax.axis_index("sp")]).astype(jnp.int32)
    docs = documents.reshape(1, tokens)
    bias = jnp.pad(
        offset_bias, ((0, 0), (0, 0), (0, BIAS_ROWS - 2 * WIN_ROWS + 1), (0, GRID_W - 2 * WIN_COLS + 1))
    ).reshape(LAYERS, heads, BIAS_ROWS * GRID_W)

    stream = lax.all_gather(grid_in, "tp", axis=0)
    query, kv = call(
        first_heads,
        (struct((tokens, cols), bf16), struct((tokens + pad, 2 * cols), bf16)),
        [VMEM] * 6,
        "first_heads",
    )(stream, of(pre_gain, 0), docs, of(query_weight, 0), of(key_weight, 0), of(value_weight, 0))
    low, high = neighbours(kv)
    doc_rows = (low[tokens:], kv[tokens:], high[tokens:])

    def attention(layer, query, kv, low, high):
        return call(
            functools.partial(attend, layer, all_rows),
            struct((tokens, cols), bf16),
            [SMEM] + [VMEM] * 8,
            "attend%d" % layer,
        )(at, query, kv, low, high, *doc_rows, bias)

    attended = lax.all_gather(attention(0, query, kv, low, high), "tp", axis=0)
    branch = call(first_out, struct((tokens + pad, feat), bf16), [VMEM] * 3, "first_out")(
        attended, of(out_weight, 0), of(post_gain, 0)
    )
    branch = lax.all_gather(branch, "tp", axis=0)
    query, kv, own = call(
        next_heads,
        (
            struct((tokens, cols), bf16),
            struct((tokens, 2 * cols), bf16),
            struct((tokens, feat), bf16),
        ),
        [SMEM] + [VMEM] * 7,
        "next_heads",
    )(
        at,
        stream,
        branch,
        of(pre_gain, 1),
        of(post_gain, 0),
        of(query_weight, 1),
        of(key_weight, 1),
        of(value_weight, 1),
    )
    low, high = neighbours(kv)
    attended = lax.all_gather(attention(1, query, kv, low, high), "tp", axis=0)
    branch, squares = call(
        last_out,
        (struct((tokens, feat), f32), struct((members, 1, tokens), f32)),
        [VMEM] * 2,
        "last_out",
    )(attended, of(out_weight, 1))
    squares = lax.all_to_all(squares, "tp", 0, 0, tiled=True)
    return call(
        functools.partial(finish, model_width), jax.ShapeDtypeStruct((tokens, feat), bf16), [VMEM] * 4, "finish"
    )(squares, branch, own, of(post_gain, 1))


def solution(mesh):
    return jax.shard_map(
        shards,
        mesh=mesh,
        in_specs=(
            P("sp", "tp"),
            P("sp"),
            P(),
            P(None, None, "tp"),
            P(None, None, "tp"),
            P(None, None, "tp"),
            P(None, "tp", None, None),
            P(None, None, "tp"),
            P(None, "tp"),
        ),
        out_specs=P("sp", "tp"),
        check_vma=False,
    )
```

```python
import functools

import jax
import jax.numpy as jnp
from jax import lax
from jax.experimental import pallas as pl
from jax.experimental.pallas import tpu as pltpu
from jax.sharding import PartitionSpec as P

HEAD_DIM = 64
WIN_ROWS = 8
WIN_COLS = 16
GRID_W = 32
LAYERS = 2
EPSILON = 1e-06
RIM = WIN_ROWS // 2
BIAS_ROWS = 2 * WIN_ROWS
LOWEST = -1e30
PAD = 16

VMEM = pl.BlockSpec(memory_space=pltpu.VMEM)
SMEM = pl.BlockSpec(memory_space=pltpu.SMEM)
HBM = pl.BlockSpec(memory_space=pltpu.HBM)


def call(body, outs, specs, name, scratch=()):
    kernel = pl.pallas_call(
        body,
        out_shape=outs,
        in_specs=specs,
        out_specs=jax.tree.map(lambda _: VMEM, outs),
        scratch_shapes=scratch,
        compiler_params=pltpu.CompilerParams(vmem_limit_bytes=16 << 20),
        name=name,
    )

    def run(*args):
        return kernel(
            *(
                arg if spec is SMEM else pltpu.with_memory_space_constraint(arg, spec.memory_space)
                for arg, spec in zip(args, specs, strict=True)
            )
        )

    return run


def copying(pairs, sems):
    copies = [pltpu.make_async_copy(src, dst, sems.at[i]) for i, (src, dst) in enumerate(pairs)]
    for copy in copies:
        copy.start()
    return copies


def as_column(row, size):
    return jnp.transpose(jnp.broadcast_to(row, (size, size)))


def lanes(i, width):
    return slice(i * width, (i + 1) * width)


def key_value(scaled, scaler, wk, wv, kv_ref):
    tokens, cols = scaled.shape[0], wk.shape[1]
    both = jnp.dot(scaled, jnp.concatenate([wk, wv], axis=1), preferred_element_type=jnp.float32)
    scaler = jnp.concatenate([scaler] * (2 * cols // scaler.shape[1]), axis=1)
    kv_ref[:tokens] = (both * scaler).astype(jnp.bfloat16)


def scaler_of(squares, model_width):
    total = jnp.sum(squares, axis=1, keepdims=True)
    return jnp.broadcast_to(lax.rsqrt(total / model_width + EPSILON), squares.shape)


def first_heads(
    x_ref, gain_hbm, docs_hbm, wk_hbm, wv_hbm,
    kv_ref, scaled_ref, scaler_ref, gain_ref, docs_ref, wk_ref, wv_ref, sems,
):
    copies = copying(
        (
            (gain_hbm, gain_ref),
            (docs_hbm, docs_ref),
            (wk_hbm.at[0], wk_ref),
            (wv_hbm.at[0], wv_ref),
        ),
        sems,
    )
    count, tokens, feat = x_ref.shape
    squares = jnp.zeros((tokens, feat), jnp.float32)
    copies[0].wait()
    for i in range(count):
        wide = x_ref[i].astype(jnp.float32)
        squares += wide * wide
        scaled_ref[:, lanes(i, feat)] = (wide * gain_ref[0:1, lanes(i, feat)]).astype(jnp.bfloat16)
    scaler = scaler_of(squares, count * feat)
    scaler_ref[...] = scaler
    copies[1].wait()
    row = docs_ref[...].astype(jnp.float32)
    row = jnp.concatenate([row] * (kv_ref.shape[1] // tokens), axis=1)
    kv_ref[tokens:] = jnp.broadcast_to(row, (kv_ref.shape[0] - tokens, kv_ref.shape[1])).astype(jnp.bfloat16)
    copies[2].wait()
    copies[3].wait()
    key_value(scaled_ref[...], scaler, wk_ref[...], wv_ref[...], kv_ref)


def query_from(scaled_ref, scaler_ref, wq):
    query = jnp.dot(scaled_ref[...], wq, preferred_element_type=jnp.float32)
    return (query * scaler_ref[...]).astype(jnp.bfloat16)


def biases(last_row, first_row, flat_ref, bias_ref):
    heads, tokens, keys = bias_ref.shape
    rows = tokens // GRID_W
    width = flat_ref.shape[1]
    token = lax.broadcasted_iota(jnp.int32, (GRID_W, keys), 0)
    other = lax.broadcasted_iota(jnp.int32, (GRID_W, keys), 1)
    key_row, key_col = first_row - rows + other // GRID_W, other % GRID_W
    col_start = jnp.clip(token - WIN_COLS // 2, 0, GRID_W - WIN_COLS)
    near = (key_col >= col_start) & (key_col < col_start + WIN_COLS)
    for r in range(rows):
        row_start = jnp.clip(first_row + r - RIM, 0, last_row - WIN_ROWS)
        inside = near & (key_row >= row_start) & (key_row < row_start + WIN_ROWS)
        shift = (-(WIN_COLS - 1) - (WIN_ROWS - 1 - rows - r) * GRID_W) % width
        for head in range(heads):
            flat = jnp.broadcast_to(flat_ref[head : head + 1], (GRID_W, width))
            turned = pltpu.roll(flat, shift, 1, stride=1, stride_axis=0)[:, :keys]
            bias_ref[head, lanes(r, GRID_W)] = jnp.where(inside, turned, LOWEST)


def first_query(
    last_row, at_ref, scaled_ref, scaler_ref, flat_ref, wq_hbm, wk_hbm, wv_hbm, wo_hbm, post_hbm,
    q_ref, bias_ref, wk_ref, wv_ref, wo_ref, post_ref, wq_ref, sems,
):
    copies = copying(
        (
            (wq_hbm.at[0], wq_ref),
            (wo_hbm.at[0], wo_ref),
            (post_hbm, post_ref),
            (wk_hbm.at[1], wk_ref),
            (wv_hbm.at[1], wv_ref),
        ),
        sems,
    )
    biases(last_row, at_ref[1] * (scaled_ref.shape[0] // GRID_W), flat_ref.at[0], bias_ref)
    copies[0].wait()
    q_ref[...] = query_from(scaled_ref, scaler_ref, wq_ref[...])
    for copy in copies[1:]:
        copy.wait()


def next_query(
    last_row, at_ref, scaled_ref, scaler_ref, flat_ref, wq_hbm, wo_hbm,
    q_ref, bias_ref, wo_ref, wq_ref, sems,
):
    copies = copying(((wq_hbm.at[1], wq_ref), (wo_hbm.at[1], wo_ref)), sems)
    biases(last_row, at_ref[1] * (scaled_ref.shape[0] // GRID_W), flat_ref.at[1], bias_ref)
    copies[0].wait()
    q_ref[...] = query_from(scaled_ref, scaler_ref, wq_ref[...])
    copies[1].wait()


def next_heads(
    at_ref, x_ref, b_ref, gain_ref, post_ref, wk_ref, wv_ref, kv_ref, scaled_ref, scaler_ref, own_ref
):
    count, tokens, feat = x_ref.shape
    squares = jnp.zeros((tokens, feat), jnp.float32)
    for i in range(count):
        branch = b_ref[i, :tokens].astype(jnp.float32)
        squares += branch * branch
    scale = scaler_of(squares, count * feat)
    squares = jnp.zeros((tokens, feat), jnp.float32)
    for i in range(count):
        parts = b_ref[i, tokens:].astype(jnp.float32)
        post = parts[0:1] + parts[1:2] + parts[2:3]
        branch = b_ref[i, :tokens].astype(jnp.float32)
        stream = (x_ref[i].astype(jnp.float32) + branch * scale * post).astype(jnp.bfloat16)
        wide = stream.astype(jnp.float32)
        squares += wide * wide
        scaled_ref[:, lanes(i, feat)] = (wide * gain_ref[1:2, lanes(i, feat)]).astype(jnp.bfloat16)
    scaler = scaler_of(squares, count * feat)
    scaler_ref[...] = scaler
    at = at_ref[0]
    own = x_ref[at].astype(jnp.float32)
    own_branch = b_ref[at][:tokens].astype(jnp.float32)
    own_ref[...] = (own + own_branch * scale * post_ref[0:1]).astype(jnp.bfloat16)
    key_value(scaled_ref[...], scaler, wk_ref[...], wv_ref[...], kv_ref)


def attend(q_ref, own_ref, low_ref, high_ref, dl_ref, do_ref, dh_ref, bias_ref, out_ref):
    tokens, cols = q_ref.shape
    heads = cols // HEAD_DIM
    blocks = (low_ref, own_ref, high_ref)
    key = jnp.concatenate([b[:tokens, :cols] for b in blocks], axis=0)
    value = jnp.concatenate([b[:tokens, cols:] for b in blocks], axis=0)
    key_docs = jnp.concatenate(
        [d[:1, :tokens].astype(jnp.float32) for d in (dl_ref, do_ref, dh_ref)], axis=1
    )
    query_docs = as_column(do_ref[:1, :tokens].astype(jnp.float32), tokens)
    same = key_docs == jnp.concatenate([query_docs] * 3, axis=1)
    query = q_ref[...]
    lane = lax.broadcasted_iota(jnp.int32, (tokens, cols), 1)
    split = jnp.concatenate(
        [jnp.where(lane // HEAD_DIM == h, query, jnp.zeros_like(query)) for h in range(heads)], axis=0
    )
    products = lax.dot_general(
        split, key, (((1,), (1,)), ((), ())), preferred_element_type=jnp.float32
    )
    lifted = []
    for h in range(heads):
        scores = products[lanes(h, tokens)] * HEAD_DIM ** (-0.5) + bias_ref[h]
        scores = jnp.where(same, scores, LOWEST)
        lifted.append(jnp.exp(scores - jnp.max(scores, axis=1, keepdims=True)))
    lifted = jnp.concatenate(lifted, axis=0)
    summed = jnp.dot(lifted.astype(jnp.bfloat16), value, preferred_element_type=jnp.float32)
    summed = summed / jnp.sum(lifted, axis=1, keepdims=True)
    result = summed[:tokens]
    for h in range(1, heads):
        result = jnp.where(lane // HEAD_DIM == h, summed[lanes(h, tokens)], result)
    out_ref[...] = result.astype(jnp.bfloat16)


def projected(a_ref, w_ref):
    joined = jnp.concatenate([a_ref[i] for i in range(a_ref.shape[0])], axis=1)
    return jnp.dot(joined, w_ref[...], preferred_element_type=jnp.float32)


def first_out(a_ref, w_ref, post_ref, out_ref):
    tokens = a_ref.shape[1]
    out_ref[:tokens] = projected(a_ref, w_ref).astype(jnp.bfloat16)
    post = post_ref[0:1]
    high = post.astype(jnp.bfloat16).astype(jnp.float32)
    middle = (post - high).astype(jnp.bfloat16).astype(jnp.float32)
    low = post - high - middle
    place = lax.broadcasted_iota(jnp.int32, (out_ref.shape[0] - tokens, post.shape[1]), 0)
    rows = jnp.where(place == 0, high, jnp.where(place == 1, middle, low))
    out_ref[tokens:] = rows.astype(jnp.bfloat16)


def last_out(a_ref, w_ref, branch_ref, squares_ref):
    branch = projected(a_ref, w_ref)
    branch_ref[...] = branch
    squares = jnp.sum(jnp.transpose(branch * branch), axis=0, keepdims=True)
    squares_ref[...] = jnp.broadcast_to(squares[None], squares_ref.shape)


def finish(model_width, squares_ref, branch_ref, own_ref, post_ref, out_ref):
    total = jnp.sum(squares_ref[...], axis=0)
    scale = as_column(lax.rsqrt(total / model_width + EPSILON), branch_ref.shape[0])
    out_ref[...] = (
        own_ref[...].astype(jnp.float32) + branch_ref[...] * scale * post_ref[1:2]
    ).astype(jnp.bfloat16)


def neighbours(block):
    count = lax.axis_size("sp")
    forward = [(i, i + 1) for i in range(count - 1)]
    backward = [(i + 1, i) for i in range(count - 1)]
    return lax.ppermute(block, "sp", forward), lax.ppermute(block, "sp", backward)


def gathered(block):
    return lax.all_gather(block, "tp", axis=0)


def shards(
    grid_in,
    documents,
    pre_gain,
    query_weight,
    key_weight,
    value_weight,
    offset_bias,
    out_weight,
    post_gain,
):
    tokens, feat = grid_in.shape
    _, model_width, cols = query_weight.shape
    heads = offset_bias.shape[1]
    bf16, f32 = jnp.bfloat16, jnp.float32
    members = lax.axis_size("tp")
    all_rows = tokens // GRID_W * lax.axis_size("sp")
    at = jnp.stack([lax.axis_index("tp"), lax.axis_index("sp")]).astype(jnp.int32)
    flat = jnp.pad(
        offset_bias, ((0, 0), (0, 0), (0, BIAS_ROWS - 2 * WIN_ROWS + 1), (0, GRID_W - 2 * WIN_COLS + 1))
    ).reshape(LAYERS, heads, BIAS_ROWS * GRID_W)
    weight = pltpu.VMEM((model_width, cols), bf16)
    shared = (pltpu.VMEM((tokens, model_width), bf16), pltpu.VMEM((tokens, feat), f32))

    stream = gathered(grid_in)
    kv, scaled, scaler, gain = call(
        first_heads,
        (pltpu.VMEM((tokens + PAD, 2 * cols), bf16), *shared, pltpu.VMEM(pre_gain.shape, f32)),
        [VMEM] + [HBM] * 4,
        "first_heads",
        [pltpu.VMEM((1, tokens), jnp.int32), weight, weight, pltpu.SemaphoreType.DMA((4,))],
    )(stream, pre_gain, documents.reshape(1, tokens), key_weight, value_weight)
    low, high = neighbours(kv)
    bias_of = pltpu.VMEM((heads, tokens, 3 * tokens), f32)
    query, bias, wk, wv, out, post = call(
        functools.partial(first_query, all_rows),
        (
            pltpu.VMEM((tokens, cols), bf16),
            bias_of,
            *[weight] * 3,
            pltpu.VMEM(post_gain.shape, f32),
        ),
        [SMEM, VMEM, VMEM, VMEM] + [HBM] * 5,
        "first_query",
        [weight, pltpu.SemaphoreType.DMA((5,))],
    )(at, scaled, scaler, flat, query_weight, key_weight, value_weight, out_weight, post_gain)
    doc_rows = (low[tokens:], kv[tokens:], high[tokens:])

    def attention(query, kv, low, high, bias):
        return call(attend, pltpu.VMEM((tokens, cols), bf16), [VMEM] * 8, "attend")(
            query, kv, low, high, *doc_rows, bias
        )

    attended = gathered(attention(query, kv, low, high, bias))
    branch = call(first_out, pltpu.VMEM((tokens + PAD, feat), bf16), [VMEM] * 3, "first_out")(
        attended, out, post
    )
    branch = gathered(branch)
    kv, scaled, scaler, own = call(
        next_heads,
        (pltpu.VMEM((tokens, 2 * cols), bf16), *shared, pltpu.VMEM((tokens, feat), bf16)),
        [SMEM] + [VMEM] * 6,
        "next_heads",
    )(at, stream, branch, gain, post, wk, wv)
    low, high = neighbours(kv)
    query, bias, out = call(
        functools.partial(next_query, all_rows),
        (pltpu.VMEM((tokens, cols), bf16), bias_of, weight),
        [SMEM] + [VMEM] * 3 + [HBM] * 2,
        "next_query",
        [weight, pltpu.SemaphoreType.DMA((2,))],
    )(at, scaled, scaler, flat, query_weight, out_weight)
    attended = gathered(attention(query, kv, low, high, bias))
    branch, squares = call(
        last_out,
        (pltpu.VMEM((tokens, feat), f32), pltpu.VMEM((members, 1, tokens), f32)),
        [VMEM] * 2,
        "last_out",
    )(attended, out)
    squares = lax.all_to_all(squares, "tp", 0, 0, tiled=True)
    return call(
        functools.partial(finish, model_width),
        jax.ShapeDtypeStruct((tokens, feat), bf16),
        [VMEM] * 4,
        "finish",
    )(squares, branch, own, post)


def solution(mesh):
    return jax.shard_map(
        shards,
        mesh=mesh,
        in_specs=(
            P("sp", "tp"),
            P("sp"),
            P(),
            P(None, None, "tp"),
            P(None, None, "tp"),
            P(None, None, "tp"),
            P(None, "tp", None, None),
            P(None, None, "tp"),
            P(None, "tp"),
        ),
        out_specs=P("sp", "tp"),
        check_vma=False,
    )
```

```python
import functools

import jax
import jax.numpy as jnp
from jax import lax
from jax.experimental import pallas as pl
from jax.experimental.pallas import tpu as pltpu
from jax.sharding import PartitionSpec as P

HEAD_DIM = 64
WIN_ROWS = 8
WIN_COLS = 16
GRID_W = 32
LAYERS = 2
EPSILON = 1e-06
RIM = WIN_ROWS // 2
BIAS_ROWS = 2 * WIN_ROWS
LOWEST = -1e30
PAD = 16

VMEM = pl.BlockSpec(memory_space=pltpu.VMEM)
HBM = pl.BlockSpec(memory_space=pltpu.HBM)


def call(body, outs, specs, name, scratch=()):
    kernel = pl.pallas_call(
        body,
        out_shape=outs,
        in_specs=specs,
        out_specs=jax.tree.map(lambda _: VMEM, outs),
        scratch_shapes=scratch,
        compiler_params=pltpu.CompilerParams(vmem_limit_bytes=16 << 20),
        name=name,
    )

    def run(*args):
        return kernel(
            *(
                pltpu.with_memory_space_constraint(arg, spec.memory_space)
                for arg, spec in zip(args, specs, strict=True)
            )
        )

    return run


def copying(pairs, sems):
    copies = [pltpu.make_async_copy(src, dst, sems.at[i]) for i, (src, dst) in enumerate(pairs)]
    for copy in copies:
        copy.start()
    return copies


def as_column(row, size):
    return jnp.transpose(jnp.broadcast_to(row, (size, size)))


def lanes(i, width):
    return slice(i * width, (i + 1) * width)


def key_value(scaled, scaler, wk, wv, kv_ref):
    tokens, cols = scaled.shape[0], wk.shape[1]
    both = jnp.dot(scaled, jnp.concatenate([wk, wv], axis=1), preferred_element_type=jnp.float32)
    scaler = jnp.concatenate([scaler] * (2 * cols // scaler.shape[1]), axis=1)
    kv_ref[:tokens] = (both * scaler).astype(jnp.bfloat16)


def scaler_of(squares, model_width):
    total = jnp.sum(squares, axis=1, keepdims=True)
    return jnp.broadcast_to(lax.rsqrt(total / model_width + EPSILON), squares.shape)


def first_heads(
    x_ref, gain_hbm, docs_hbm, wk_hbm, wv_hbm,
    kv_ref, scaled_ref, scaler_ref, gain_ref, docs_ref, wk_ref, wv_ref, sems,
):
    copies = copying(
        (
            (gain_hbm, gain_ref),
            (docs_hbm, docs_ref),
            (wk_hbm.at[0], wk_ref),
            (wv_hbm.at[0], wv_ref),
        ),
        sems,
    )
    count, tokens, feat = x_ref.shape
    squares = jnp.zeros((tokens, feat), jnp.float32)
    copies[0].wait()
    for i in range(count):
        wide = x_ref[i].astype(jnp.float32)
        squares += wide * wide
        scaled_ref[:, lanes(i, feat)] = (wide * gain_ref[0:1, lanes(i, feat)]).astype(jnp.bfloat16)
    scaler = scaler_of(squares, count * feat)
    scaler_ref[...] = scaler
    copies[1].wait()
    row = docs_ref[...].astype(jnp.float32)
    row = jnp.concatenate([row] * (kv_ref.shape[1] // tokens), axis=1)
    kv_ref[tokens:] = jnp.broadcast_to(row, (kv_ref.shape[0] - tokens, kv_ref.shape[1])).astype(jnp.bfloat16)
    copies[2].wait()
    copies[3].wait()
    key_value(scaled_ref[...], scaler, wk_ref[...], wv_ref[...], kv_ref)


def query_from(scaled_ref, scaler_ref, wq):
    query = jnp.dot(scaled_ref[...], wq, preferred_element_type=jnp.float32)
    return (query * scaler_ref[...]).astype(jnp.bfloat16)


def biases(last_row, block, flat_ref, bias_ref):
    blocks, heads, tokens, _ = bias_ref.shape
    rows = tokens // GRID_W
    first_row = block * rows
    width = flat_ref.shape[1]
    token = lax.broadcasted_iota(jnp.int32, (GRID_W, tokens), 0)
    other = lax.broadcasted_iota(jnp.int32, (GRID_W, tokens), 1)
    row, col = other // GRID_W, other % GRID_W
    col_start = jnp.clip(token - WIN_COLS // 2, 0, GRID_W - WIN_COLS)
    near = (col >= col_start) & (col < col_start + WIN_COLS)
    for head in range(heads):
        flat = jnp.broadcast_to(flat_ref[head : head + 1], (GRID_W, width))
        turned = pltpu.roll(flat, width - (WIN_COLS - 1), 1, stride=1, stride_axis=0)
        for r in range(rows):
            start = jnp.clip(first_row + r - RIM, 0, last_row - WIN_ROWS) - first_row
            skipped = (WIN_ROWS - 1 - rows - r) * GRID_W
            for j in range(blocks):
                key_row = row + (j - 1) * rows
                inside = near & (key_row >= start) & (key_row < start + WIN_ROWS)
                part = turned[:, skipped + j * tokens : skipped + (j + 1) * tokens]
                place = jnp.where(block % 2 == 0, j, blocks - 1 - j)
                bias_ref[place, head, lanes(r, GRID_W)] = jnp.where(inside, part, LOWEST)


def first_query(
    last_row, scaled_ref, scaler_ref, flat_ref, wq_hbm, wk_hbm, wv_hbm, wo_hbm, post_hbm,
    q_ref, bias_ref, wk_ref, wv_ref, wo_ref, post_ref, wq_ref, sems,
):
    copies = copying(
        (
            (wq_hbm.at[0], wq_ref),
            (wo_hbm.at[0], wo_ref),
            (post_hbm, post_ref),
            (wk_hbm.at[1], wk_ref),
            (wv_hbm.at[1], wv_ref),
        ),
        sems,
    )
    biases(last_row, lax.axis_index("sp"), flat_ref.at[0], bias_ref)
    copies[0].wait()
    q_ref[...] = query_from(scaled_ref, scaler_ref, wq_ref[...])
    for copy in copies[1:]:
        copy.wait()


def next_query(
    last_row, scaled_ref, scaler_ref, flat_ref, wq_hbm, wo_hbm,
    q_ref, bias_ref, wo_ref, wq_ref, sems,
):
    copies = copying(((wq_hbm.at[1], wq_ref), (wo_hbm.at[1], wo_ref)), sems)
    biases(last_row, lax.axis_index("sp"), flat_ref.at[1], bias_ref)
    copies[0].wait()
    q_ref[...] = query_from(scaled_ref, scaler_ref, wq_ref[...])
    copies[1].wait()


def next_heads(
    x_ref, b_ref, gain_ref, post_ref, wk_ref, wv_ref, kv_ref, scaled_ref, scaler_ref, own_ref
):
    count, tokens, feat = x_ref.shape
    squares = jnp.zeros((tokens, feat), jnp.float32)
    for i in range(count):
        branch = b_ref[i, :tokens].astype(jnp.float32)
        squares += branch * branch
    scale = scaler_of(squares, count * feat)
    squares = jnp.zeros((tokens, feat), jnp.float32)
    for i in range(count):
        parts = b_ref[i, tokens:].astype(jnp.float32)
        post = parts[0:1] + parts[1:2] + parts[2:3]
        branch = b_ref[i, :tokens].astype(jnp.float32)
        stream = (x_ref[i].astype(jnp.float32) + branch * scale * post).astype(jnp.bfloat16)
        wide = stream.astype(jnp.float32)
        squares += wide * wide
        scaled_ref[:, lanes(i, feat)] = (wide * gain_ref[1:2, lanes(i, feat)]).astype(jnp.bfloat16)
    scaler = scaler_of(squares, count * feat)
    scaler_ref[...] = scaler
    at = lax.axis_index("tp")
    own = x_ref[at].astype(jnp.float32)
    own_branch = b_ref[at][:tokens].astype(jnp.float32)
    own_ref[...] = (own + own_branch * scale * post_ref[0:1]).astype(jnp.bfloat16)
    key_value(scaled_ref[...], scaler, wk_ref[...], wv_ref[...], kv_ref)


def attend(q_ref, own_ref, cross_ref, within_ref, dc_ref, do_ref, dw_ref, bias_ref, out_ref):
    tokens, cols = q_ref.shape
    heads = cols // HEAD_DIM
    blocks = (cross_ref, own_ref, within_ref)
    key = jnp.concatenate([b[:tokens, :cols] for b in blocks], axis=0)
    value = jnp.concatenate([b[:tokens, cols:] for b in blocks], axis=0)
    key_docs = jnp.concatenate(
        [d[:1, :tokens].astype(jnp.float32) for d in (dc_ref, do_ref, dw_ref)], axis=1
    )
    query_docs = as_column(do_ref[:1, :tokens].astype(jnp.float32), tokens)
    same = key_docs == jnp.concatenate([query_docs] * 3, axis=1)
    query = q_ref[...]
    lane = lax.broadcasted_iota(jnp.int32, (tokens, cols), 1)
    split = jnp.concatenate(
        [jnp.where(lane // HEAD_DIM == h, query, jnp.zeros_like(query)) for h in range(heads)], axis=0
    )
    products = lax.dot_general(
        split, key, (((1,), (1,)), ((), ())), preferred_element_type=jnp.float32
    )
    bias = [jnp.concatenate([bias_ref[j, h] for j in range(len(blocks))], axis=1) for h in range(heads)]
    lifted = []
    for h in range(heads):
        scores = products[lanes(h, tokens)] * HEAD_DIM ** (-0.5) + bias[h]
        scores = jnp.where(same, scores, LOWEST)
        lifted.append(jnp.exp(scores - jnp.max(scores, axis=1, keepdims=True)))
    lifted = jnp.concatenate(lifted, axis=0)
    summed = jnp.dot(lifted.astype(jnp.bfloat16), value, preferred_element_type=jnp.float32)
    summed = summed / jnp.sum(lifted, axis=1, keepdims=True)
    result = summed[:tokens]
    for h in range(1, heads):
        result = jnp.where(lane // HEAD_DIM == h, summed[lanes(h, tokens)], result)
    out_ref[...] = result.astype(jnp.bfloat16)


def projected(a_ref, w_ref):
    joined = jnp.concatenate([a_ref[i] for i in range(a_ref.shape[0])], axis=1)
    return jnp.dot(joined, w_ref[...], preferred_element_type=jnp.float32)


def first_out(a_ref, w_ref, post_ref, out_ref):
    tokens = a_ref.shape[1]
    out_ref[:tokens] = projected(a_ref, w_ref).astype(jnp.bfloat16)
    post = post_ref[0:1]
    high = post.astype(jnp.bfloat16).astype(jnp.float32)
    middle = (post - high).astype(jnp.bfloat16).astype(jnp.float32)
    low = post - high - middle
    place = lax.broadcasted_iota(jnp.int32, (out_ref.shape[0] - tokens, post.shape[1]), 0)
    rows = jnp.where(place == 0, high, jnp.where(place == 1, middle, low))
    out_ref[tokens:] = rows.astype(jnp.bfloat16)


def last_out(a_ref, w_ref, branch_ref, squares_ref):
    branch = projected(a_ref, w_ref)
    branch_ref[...] = branch
    squares = jnp.sum(jnp.transpose(branch * branch), axis=0, keepdims=True)
    squares_ref[...] = jnp.broadcast_to(squares[None], squares_ref.shape)


def finish(model_width, squares_ref, branch_ref, own_ref, post_ref, out_ref):
    total = jnp.sum(squares_ref[...], axis=0)
    scale = as_column(lax.rsqrt(total / model_width + EPSILON), branch_ref.shape[0])
    out_ref[...] = (
        own_ref[...].astype(jnp.float32) + branch_ref[...] * scale * post_ref[1:2]
    ).astype(jnp.bfloat16)


def neighbours(block):
    count = lax.axis_size("sp")
    edges = [[(i, i + 1), (i + 1, i)] for i in range(count - 1)]
    crossing = [pair for edge in edges[1::2] for pair in edge]
    within = [pair for edge in edges[0::2] for pair in edge]
    return lax.ppermute(block, "sp", crossing), lax.ppermute(block, "sp", within)


def gathered(block):
    return lax.all_gather(block, "tp", axis=0)


def shards(
    grid_in,
    documents,
    pre_gain,
    query_weight,
    key_weight,
    value_weight,
    offset_bias,
    out_weight,
    post_gain,
):
    tokens, feat = grid_in.shape
    _, model_width, cols = query_weight.shape
    heads = offset_bias.shape[1]
    bf16, f32 = jnp.bfloat16, jnp.float32
    members = lax.axis_size("tp")
    all_rows = tokens // GRID_W * lax.axis_size("sp")
    flat = jnp.pad(
        offset_bias, ((0, 0), (0, 0), (0, BIAS_ROWS - 2 * WIN_ROWS + 1), (0, GRID_W - 2 * WIN_COLS + 1))
    ).reshape(LAYERS, heads, BIAS_ROWS * GRID_W)
    weight = pltpu.VMEM((model_width, cols), bf16)
    shared = (pltpu.VMEM((tokens, model_width), bf16), pltpu.VMEM((tokens, feat), f32))

    stream = gathered(grid_in)
    kv, scaled, scaler, gain = call(
        first_heads,
        (pltpu.VMEM((tokens + PAD, 2 * cols), bf16), *shared, pltpu.VMEM(pre_gain.shape, f32)),
        [VMEM] + [HBM] * 4,
        "first_heads",
        [pltpu.VMEM((1, tokens), jnp.int32), weight, weight, pltpu.SemaphoreType.DMA((4,))],
    )(stream, pre_gain, documents.reshape(1, tokens), key_weight, value_weight)
    cross, within = neighbours(kv)
    bias_of = pltpu.VMEM((3, heads, tokens, tokens), f32)
    query, bias, wk, wv, out, post = call(
        functools.partial(first_query, all_rows),
        (
            pltpu.VMEM((tokens, cols), bf16),
            bias_of,
            *[weight] * 3,
            pltpu.VMEM(post_gain.shape, f32),
        ),
        [VMEM] * 3 + [HBM] * 5,
        "first_query",
        [weight, pltpu.SemaphoreType.DMA((5,))],
    )(scaled, scaler, flat, query_weight, key_weight, value_weight, out_weight, post_gain)
    doc_rows = (cross[tokens:], kv[tokens:], within[tokens:])

    def attention(query, kv, cross, within, bias):
        return call(attend, pltpu.VMEM((tokens, cols), bf16), [VMEM] * 8, "attend")(
            query, kv, cross, within, *doc_rows, bias
        )

    attended = gathered(attention(query, kv, cross, within, bias))
    branch = call(first_out, pltpu.VMEM((tokens + PAD, feat), bf16), [VMEM] * 3, "first_out")(
        attended, out, post
    )
    branch = gathered(branch)
    kv, scaled, scaler, own = call(
        next_heads,
        (pltpu.VMEM((tokens, 2 * cols), bf16), *shared, pltpu.VMEM((tokens, feat), bf16)),
        [VMEM] * 6,
        "next_heads",
    )(stream, branch, gain, post, wk, wv)
    cross, within = neighbours(kv)
    query, bias, out = call(
        functools.partial(next_query, all_rows),
        (pltpu.VMEM((tokens, cols), bf16), bias_of, weight),
        [VMEM] * 3 + [HBM] * 2,
        "next_query",
        [weight, pltpu.SemaphoreType.DMA((2,))],
    )(scaled, scaler, flat, query_weight, out_weight)
    attended = gathered(attention(query, kv, cross, within, bias))
    branch, squares = call(
        last_out,
        (pltpu.VMEM((tokens, feat), f32), pltpu.VMEM((members, 1, tokens), f32)),
        [VMEM] * 2,
        "last_out",
    )(attended, out)
    squares = lax.all_to_all(squares, "tp", 0, 0, tiled=True)
    return call(
        functools.partial(finish, model_width),
        jax.ShapeDtypeStruct((tokens, feat), bf16),
        [VMEM] * 4,
        "finish",
    )(squares, branch, own, post)


def solution(mesh):
    return jax.shard_map(
        shards,
        mesh=mesh,
        in_specs=(
            P("sp", "tp"),
            P("sp"),
            P(),
            P(None, None, "tp"),
            P(None, None, "tp"),
            P(None, None, "tp"),
            P(None, "tp", None, None),
            P(None, None, "tp"),
            P(None, "tp"),
        ),
        out_specs=P("sp", "tp"),
        check_vma=False,
    )
```

```python
import functools

import jax
import jax.numpy as jnp
from jax import lax
from jax.experimental import pallas as pl
from jax.experimental.pallas import tpu as pltpu
from jax.sharding import PartitionSpec as P

HEAD_DIM = 64
WIN_ROWS = 8
WIN_COLS = 16
GRID_W = 32
LAYERS = 2
EPSILON = 1e-06
RIM = WIN_ROWS // 2
BIAS_ROWS = 2 * WIN_ROWS
LOWEST = -1e30
PAD = 16

VMEM = pl.BlockSpec(memory_space=pltpu.VMEM)
HBM = pl.BlockSpec(memory_space=pltpu.HBM)


def call(body, outs, specs, name, scratch=()):
    kernel = pl.pallas_call(
        body,
        out_shape=outs,
        in_specs=specs,
        out_specs=jax.tree.map(lambda _: VMEM, outs),
        scratch_shapes=scratch,
        compiler_params=pltpu.CompilerParams(vmem_limit_bytes=16 << 20),
        name=name,
    )

    def run(*args):
        return kernel(
            *(
                pltpu.with_memory_space_constraint(arg, spec.memory_space)
                for arg, spec in zip(args, specs, strict=True)
            )
        )

    return run


def copying(pairs, sems):
    copies = [pltpu.make_async_copy(src, dst, sems.at[i]) for i, (src, dst) in enumerate(pairs)]
    for copy in copies:
        copy.start()
    return copies


def as_column(row, size):
    return jnp.transpose(jnp.broadcast_to(row, (size, size)))


def lanes(i, width):
    return slice(i * width, (i + 1) * width)


def key_value(scaled, scaler, wk, wv, kv_ref):
    tokens, cols = scaled.shape[0], wk.shape[1]
    both = jnp.dot(scaled, jnp.concatenate([wk, wv], axis=1), preferred_element_type=jnp.float32)
    scaler = jnp.concatenate([scaler] * (2 * cols // scaler.shape[1]), axis=1)
    kv_ref[:tokens] = (both * scaler).astype(jnp.bfloat16)


def scaler_of(squares, model_width):
    total = jnp.sum(squares, axis=1, keepdims=True)
    return jnp.broadcast_to(lax.rsqrt(total / model_width + EPSILON), squares.shape)


def first_heads(
    x_ref, gain_hbm, docs_hbm, wk_hbm, wv_hbm,
    kv_ref, scaled_ref, scaler_ref, gain_ref, docs_ref, wk_ref, wv_ref, sems,
):
    copies = copying(
        (
            (gain_hbm, gain_ref),
            (docs_hbm, docs_ref),
            (wk_hbm.at[0], wk_ref),
            (wv_hbm.at[0], wv_ref),
        ),
        sems,
    )
    count, tokens, feat = x_ref.shape
    squares = jnp.zeros((tokens, feat), jnp.float32)
    copies[0].wait()
    for i in range(count):
        wide = x_ref[i].astype(jnp.float32)
        squares += wide * wide
        scaled_ref[:, lanes(i, feat)] = (wide * gain_ref[0:1, lanes(i, feat)]).astype(jnp.bfloat16)
    scaler = scaler_of(squares, count * feat)
    scaler_ref[...] = scaler
    copies[1].wait()
    row = docs_ref[...].astype(jnp.float32)
    row = jnp.concatenate([row] * (kv_ref.shape[1] // tokens), axis=1)
    kv_ref[tokens:] = jnp.broadcast_to(row, (kv_ref.shape[0] - tokens, kv_ref.shape[1])).astype(jnp.bfloat16)
    copies[2].wait()
    copies[3].wait()
    key_value(scaled_ref[...], scaler, wk_ref[...], wv_ref[...], kv_ref)


def query_from(scaled_ref, scaler_ref, wq):
    query = jnp.dot(scaled_ref[...], wq, preferred_element_type=jnp.float32)
    return (query * scaler_ref[...]).astype(jnp.bfloat16)


def biases(last_row, block, flat_ref, bias_ref):
    blocks, heads, tokens, _ = bias_ref.shape
    rows = tokens // GRID_W
    first_row = block * rows
    width = flat_ref.shape[1]
    token = lax.broadcasted_iota(jnp.int32, (GRID_W, tokens), 0)
    other = lax.broadcasted_iota(jnp.int32, (GRID_W, tokens), 1)
    row, col = other // GRID_W, other % GRID_W
    col_start = jnp.clip(token - WIN_COLS // 2, 0, GRID_W - WIN_COLS)
    near = (col >= col_start) & (col < col_start + WIN_COLS)
    for head in range(heads):
        flat = jnp.broadcast_to(flat_ref[head : head + 1], (GRID_W, width))
        turned = pltpu.roll(flat, width - (WIN_COLS - 1), 1, stride=1, stride_axis=0)
        for r in range(rows):
            start = jnp.clip(first_row + r - RIM, 0, last_row - WIN_ROWS) - first_row
            skipped = (WIN_ROWS - 1 - rows - r) * GRID_W
            for j in range(blocks):
                key_row = row + (j - 1) * rows
                inside = near & (key_row >= start) & (key_row < start + WIN_ROWS)
                part = turned[:, skipped + j * tokens : skipped + (j + 1) * tokens]
                place = jnp.where(block % 2 == 0, j, blocks - 1 - j)
                bias_ref[place, head, lanes(r, GRID_W)] = jnp.where(inside, part, LOWEST)


def first_query(
    last_row, scaled_ref, scaler_ref, flat_ref, wq_hbm, wk_hbm, wv_hbm, wo_hbm, post_hbm,
    q_ref, bias_ref, wk_ref, wv_ref, wo_ref, post_ref, wq_ref, sems,
):
    copies = copying(
        (
            (wq_hbm.at[0], wq_ref),
            (wo_hbm.at[0], wo_ref),
            (post_hbm, post_ref),
            (wk_hbm.at[1], wk_ref),
            (wv_hbm.at[1], wv_ref),
        ),
        sems,
    )
    biases(last_row, lax.axis_index("sp"), flat_ref.at[0], bias_ref)
    copies[0].wait()
    q_ref[...] = query_from(scaled_ref, scaler_ref, wq_ref[...])
    for copy in copies[1:]:
        copy.wait()


def next_query(
    last_row, scaled_ref, scaler_ref, flat_ref, wq_hbm, wo_hbm,
    q_ref, bias_ref, wo_ref, wq_ref, sems,
):
    copies = copying(((wq_hbm.at[1], wq_ref), (wo_hbm.at[1], wo_ref)), sems)
    biases(last_row, lax.axis_index("sp"), flat_ref.at[1], bias_ref)
    copies[0].wait()
    q_ref[...] = query_from(scaled_ref, scaler_ref, wq_ref[...])
    copies[1].wait()


def next_heads(
    x_ref, b_ref, gain_ref, post_ref, wk_ref, wv_ref, kv_ref, scaled_ref, scaler_ref, own_ref
):
    count, tokens, feat = x_ref.shape
    squares = jnp.zeros((tokens, feat), jnp.float32)
    for i in range(count):
        branch = b_ref[i, :tokens].astype(jnp.float32)
        squares += branch * branch
    scale = scaler_of(squares, count * feat)
    squares = jnp.zeros((tokens, feat), jnp.float32)
    for i in range(count):
        parts = b_ref[i, tokens:].astype(jnp.float32)
        post = parts[0:1] + parts[1:2] + parts[2:3]
        branch = b_ref[i, :tokens].astype(jnp.float32)
        stream = (x_ref[i].astype(jnp.float32) + branch * scale * post).astype(jnp.bfloat16)
        wide = stream.astype(jnp.float32)
        squares += wide * wide
        scaled_ref[:, lanes(i, feat)] = (wide * gain_ref[1:2, lanes(i, feat)]).astype(jnp.bfloat16)
    scaler = scaler_of(squares, count * feat)
    scaler_ref[...] = scaler
    at = lax.axis_index("tp")
    own = x_ref[at].astype(jnp.float32)
    own_branch = b_ref[at][:tokens].astype(jnp.float32)
    own_ref[...] = (own + own_branch * scale * post_ref[0:1]).astype(jnp.bfloat16)
    key_value(scaled_ref[...], scaler, wk_ref[...], wv_ref[...], kv_ref)


def attend(q_ref, own_ref, cross_ref, within_ref, dc_ref, do_ref, dw_ref, bias_ref, out_ref):
    tokens, cols = q_ref.shape
    heads = cols // HEAD_DIM
    blocks = (cross_ref, own_ref, within_ref)
    key = jnp.concatenate([b[:tokens, :cols] for b in blocks], axis=0)
    value = jnp.concatenate([b[:tokens, cols:] for b in blocks], axis=0)
    key_docs = jnp.concatenate(
        [d[:1, :tokens].astype(jnp.float32) for d in (dc_ref, do_ref, dw_ref)], axis=1
    )
    query_docs = as_column(do_ref[:1, :tokens].astype(jnp.float32), tokens)
    same = key_docs == jnp.concatenate([query_docs] * 3, axis=1)
    query = q_ref[...]
    lane = lax.broadcasted_iota(jnp.int32, (tokens, cols), 1)
    split = jnp.concatenate(
        [jnp.where(lane // HEAD_DIM == h, query, jnp.zeros_like(query)) for h in range(heads)], axis=0
    )
    products = lax.dot_general(
        split, key, (((1,), (1,)), ((), ())), preferred_element_type=jnp.float32
    )
    bias = [jnp.concatenate([bias_ref[j, h] for j in range(len(blocks))], axis=1) for h in range(heads)]
    lifted = []
    for h in range(heads):
        scores = products[lanes(h, tokens)] * HEAD_DIM ** (-0.5) + bias[h]
        scores = jnp.where(same, scores, LOWEST)
        lifted.append(jnp.exp(scores - jnp.max(scores, axis=1, keepdims=True)))
    lifted = jnp.concatenate(lifted, axis=0)
    summed = jnp.dot(lifted.astype(jnp.bfloat16), value, preferred_element_type=jnp.float32)
    summed = summed / jnp.sum(lifted, axis=1, keepdims=True)
    result = summed[:tokens]
    for h in range(1, heads):
        result = jnp.where(lane // HEAD_DIM == h, summed[lanes(h, tokens)], result)
    out_ref[...] = jnp.broadcast_to(result.astype(jnp.bfloat16)[None], out_ref.shape)


def projected(a_ref, w_ref):
    joined = jnp.concatenate([a_ref[place(i, a_ref.shape[0])] for i in range(a_ref.shape[0])], axis=1)
    return jnp.dot(joined, w_ref[...], preferred_element_type=jnp.float32)


def first_out(a_ref, w_ref, post_ref, out_ref):
    tokens = a_ref.shape[1]
    out_ref[:tokens] = projected(a_ref, w_ref).astype(jnp.bfloat16)
    post = post_ref[0:1]
    high = post.astype(jnp.bfloat16).astype(jnp.float32)
    middle = (post - high).astype(jnp.bfloat16).astype(jnp.float32)
    low = post - high - middle
    place = lax.broadcasted_iota(jnp.int32, (out_ref.shape[0] - tokens, post.shape[1]), 0)
    rows = jnp.where(place == 0, high, jnp.where(place == 1, middle, low))
    out_ref[tokens:] = rows.astype(jnp.bfloat16)


def last_out(a_ref, w_ref, branch_ref, squares_ref):
    branch = projected(a_ref, w_ref)
    branch_ref[...] = branch
    squares = jnp.sum(jnp.transpose(branch * branch), axis=0, keepdims=True)
    squares_ref[...] = jnp.broadcast_to(squares[None], squares_ref.shape)


def finish(model_width, squares_ref, branch_ref, own_ref, post_ref, out_ref):
    total = jnp.sum(squares_ref[...], axis=0)
    scale = as_column(lax.rsqrt(total / model_width + EPSILON), branch_ref.shape[0])
    out_ref[...] = (
        own_ref[...].astype(jnp.float32) + branch_ref[...] * scale * post_ref[1:2]
    ).astype(jnp.bfloat16)


def neighbours(block):
    count = lax.axis_size("sp")
    edges = [[(i, i + 1), (i + 1, i)] for i in range(count - 1)]
    crossing = [pair for edge in edges[1::2] for pair in edge]
    within = [pair for edge in edges[0::2] for pair in edge]
    return lax.ppermute(block, "sp", crossing), lax.ppermute(block, "sp", within)


def gathered(block):
    return lax.all_gather(block, "tp", axis=0)


def place(index, count):
    return index % 2 * (count // 2) + index // 2


def gathered_by_core(copies):
    chips = copies.shape[0]
    across = [[core + 2 * chip for chip in range(chips)] for core in range(2)]
    pairs = [[2 * chip, 2 * chip + 1] for chip in range(chips)]
    same = lax.all_to_all(copies, "tp", 0, 0, axis_index_groups=across, tiled=True)
    both = lax.all_gather(same, "tp", axis=0, axis_index_groups=pairs)
    return both.reshape(2 * chips, *copies.shape[1:])


def shards(
    grid_in,
    documents,
    pre_gain,
    query_weight,
    key_weight,
    value_weight,
    offset_bias,
    out_weight,
    post_gain,
):
    tokens, feat = grid_in.shape
    _, model_width, cols = query_weight.shape
    heads = offset_bias.shape[1]
    bf16, f32 = jnp.bfloat16, jnp.float32
    members = lax.axis_size("tp")
    all_rows = tokens // GRID_W * lax.axis_size("sp")
    flat = jnp.pad(
        offset_bias, ((0, 0), (0, 0), (0, BIAS_ROWS - 2 * WIN_ROWS + 1), (0, GRID_W - 2 * WIN_COLS + 1))
    ).reshape(LAYERS, heads, BIAS_ROWS * GRID_W)
    weight = pltpu.VMEM((model_width, cols), bf16)
    shared = (pltpu.VMEM((tokens, model_width), bf16), pltpu.VMEM((tokens, feat), f32))

    stream = gathered(grid_in)
    kv, scaled, scaler, gain = call(
        first_heads,
        (pltpu.VMEM((tokens + PAD, 2 * cols), bf16), *shared, pltpu.VMEM(pre_gain.shape, f32)),
        [VMEM] + [HBM] * 4,
        "first_heads",
        [pltpu.VMEM((1, tokens), jnp.int32), weight, weight, pltpu.SemaphoreType.DMA((4,))],
    )(stream, pre_gain, documents.reshape(1, tokens), key_weight, value_weight)
    cross, within = neighbours(kv)
    bias_of = pltpu.VMEM((3, heads, tokens, tokens), f32)
    query, bias, wk, wv, out, post = call(
        functools.partial(first_query, all_rows),
        (
            pltpu.VMEM((tokens, cols), bf16),
            bias_of,
            *[weight] * 3,
            pltpu.VMEM(post_gain.shape, f32),
        ),
        [VMEM] * 3 + [HBM] * 5,
        "first_query",
        [weight, pltpu.SemaphoreType.DMA((5,))],
    )(scaled, scaler, flat, query_weight, key_weight, value_weight, out_weight, post_gain)
    doc_rows = (cross[tokens:], kv[tokens:], within[tokens:])

    def attention(query, kv, cross, within, bias):
        return call(attend, pltpu.VMEM((members // 2, tokens, cols), bf16), [VMEM] * 8, "attend")(
            query, kv, cross, within, *doc_rows, bias
        )

    attended = gathered_by_core(attention(query, kv, cross, within, bias))
    branch = call(first_out, pltpu.VMEM((tokens + PAD, feat), bf16), [VMEM] * 3, "first_out")(
        attended, out, post
    )
    branch = gathered(branch)
    kv, scaled, scaler, own = call(
        next_heads,
        (pltpu.VMEM((tokens, 2 * cols), bf16), *shared, pltpu.VMEM((tokens, feat), bf16)),
        [VMEM] * 6,
        "next_heads",
    )(stream, branch, gain, post, wk, wv)
    cross, within = neighbours(kv)
    query, bias, out = call(
        functools.partial(next_query, all_rows),
        (pltpu.VMEM((tokens, cols), bf16), bias_of, weight),
        [VMEM] * 3 + [HBM] * 2,
        "next_query",
        [weight, pltpu.SemaphoreType.DMA((2,))],
    )(scaled, scaler, flat, query_weight, out_weight)
    attended = gathered_by_core(attention(query, kv, cross, within, bias))
    branch, squares = call(
        last_out,
        (pltpu.VMEM((tokens, feat), f32), pltpu.VMEM((members, 1, tokens), f32)),
        [VMEM] * 2,
        "last_out",
    )(attended, out)
    squares = lax.all_to_all(squares, "tp", 0, 0, tiled=True)
    return call(
        functools.partial(finish, model_width),
        jax.ShapeDtypeStruct((tokens, feat), bf16),
        [VMEM] * 4,
        "finish",
    )(squares, branch, own, post)


def solution(mesh):
    return jax.shard_map(
        shards,
        mesh=mesh,
        in_specs=(
            P("sp", "tp"),
            P("sp"),
            P(),
            P(None, None, "tp"),
            P(None, None, "tp"),
            P(None, None, "tp"),
            P(None, "tp", None, None),
            P(None, None, "tp"),
            P(None, "tp"),
        ),
        out_specs=P("sp", "tp"),
        check_vma=False,
    )
```

```python
import functools

import jax
import jax.numpy as jnp
from jax import lax
from jax.experimental import pallas as pl
from jax.experimental.pallas import tpu as pltpu
from jax.sharding import PartitionSpec as P

HEAD_DIM = 64
WIN_ROWS = 8
WIN_COLS = 16
GRID_W = 32
LAYERS = 2
EPSILON = 1e-06
RIM = WIN_ROWS // 2
BIAS_ROWS = 2 * WIN_ROWS
LOWEST = -1e30
PAD = 16
CHUNKS = 2

VMEM = pl.BlockSpec(memory_space=pltpu.VMEM)
HBM = pl.BlockSpec(memory_space=pltpu.HBM)


def call(body, outs, specs, name, scratch=()):
    kernel = pl.pallas_call(
        body,
        out_shape=outs,
        in_specs=specs,
        out_specs=jax.tree.map(lambda _: VMEM, outs),
        scratch_shapes=scratch,
        compiler_params=pltpu.CompilerParams(vmem_limit_bytes=16 << 20),
        name=name,
    )

    def run(*args):
        return kernel(
            *(
                pltpu.with_memory_space_constraint(arg, spec.memory_space)
                for arg, spec in zip(args, specs, strict=True)
            )
        )

    return run


def copying(pairs, sems):
    copies = [pltpu.make_async_copy(src, dst, sems.at[i]) for i, (src, dst) in enumerate(pairs)]
    for copy in copies:
        copy.start()
    return copies


def as_column(row, size):
    return jnp.transpose(jnp.broadcast_to(row, (size, size)))


def lanes(i, width):
    return slice(i * width, (i + 1) * width)


def key_value(scaled, scaler, wk, wv, kv_ref):
    tokens, cols = scaled.shape[0], wk.shape[1]
    both = jnp.dot(scaled, jnp.concatenate([wk, wv], axis=1), preferred_element_type=jnp.float32)
    scaler = jnp.concatenate([scaler] * (2 * cols // scaler.shape[1]), axis=1)
    kv_ref[:tokens] = (both * scaler).astype(jnp.bfloat16)


def scaler_of(squares, model_width):
    total = jnp.sum(squares, axis=1, keepdims=True)
    return jnp.broadcast_to(lax.rsqrt(total / model_width + EPSILON), squares.shape)


def first_heads(
    x_ref, gain_hbm, docs_hbm, wk_hbm, wv_hbm,
    kv_ref, scaled_ref, scaler_ref, gain_ref, docs_ref, wk_ref, wv_ref, sems,
):
    count, tokens, feat = x_ref.shape
    cols = wk_ref.shape[1]
    step = count * feat // CHUNKS
    pieces = [slice(i * step, (i + 1) * step) for i in range(CHUNKS)]
    gain_copy, *copies, docs_copy = copying(
        (
            (gain_hbm, gain_ref),
            *(
                (hbm.at[0, piece], ref.at[piece])
                for piece in pieces
                for hbm, ref in ((wk_hbm, wk_ref), (wv_hbm, wv_ref))
            ),
            (docs_hbm, docs_ref),
        ),
        sems,
    )
    squares = jnp.zeros((tokens, feat), jnp.float32)
    for i in range(count):
        wide = x_ref[i].astype(jnp.float32)
        squares += wide * wide
    scaler = scaler_of(squares, count * feat)
    scaler_ref[...] = scaler
    gain_copy.wait()
    for i in range(count):
        wide = x_ref[i].astype(jnp.float32)
        scaled_ref[:, lanes(i, feat)] = (wide * gain_ref[0:1, lanes(i, feat)]).astype(jnp.bfloat16)
    both = jnp.zeros((tokens, 2 * cols), jnp.float32)
    for i, piece in enumerate(pieces):
        copies[2 * i].wait()
        copies[2 * i + 1].wait()
        weights = jnp.concatenate([wk_ref[piece], wv_ref[piece]], axis=1)
        both += jnp.dot(scaled_ref[:, piece], weights, preferred_element_type=jnp.float32)
    scaler = jnp.concatenate([scaler] * (2 * cols // feat), axis=1)
    kv_ref[:tokens] = (both * scaler).astype(jnp.bfloat16)
    docs_copy.wait()
    row = docs_ref[...].astype(jnp.float32)
    row = jnp.concatenate([row] * (kv_ref.shape[1] // tokens), axis=1)
    kv_ref[tokens:] = jnp.broadcast_to(row, (kv_ref.shape[0] - tokens, kv_ref.shape[1])).astype(jnp.bfloat16)


def query_from(scaled_ref, scaler_ref, wq):
    query = jnp.dot(scaled_ref[...], wq, preferred_element_type=jnp.float32)
    return (query * scaler_ref[...]).astype(jnp.bfloat16)


def biases(last_row, block, flat_ref, bias_ref):
    blocks, heads, tokens, _ = bias_ref.shape
    rows = tokens // GRID_W
    first_row = block * rows
    width = flat_ref.shape[1]
    token = lax.broadcasted_iota(jnp.int32, (GRID_W, tokens), 0)
    other = lax.broadcasted_iota(jnp.int32, (GRID_W, tokens), 1)
    row, col = other // GRID_W, other % GRID_W
    col_start = jnp.clip(token - WIN_COLS // 2, 0, GRID_W - WIN_COLS)
    near = (col >= col_start) & (col < col_start + WIN_COLS)
    for head in range(heads):
        flat = jnp.broadcast_to(flat_ref[head : head + 1], (GRID_W, width))
        turned = pltpu.roll(flat, width - (WIN_COLS - 1), 1, stride=1, stride_axis=0)
        for r in range(rows):
            start = jnp.clip(first_row + r - RIM, 0, last_row - WIN_ROWS) - first_row
            skipped = (WIN_ROWS - 1 - rows - r) * GRID_W
            for j in range(blocks):
                key_row = row + (j - 1) * rows
                inside = near & (key_row >= start) & (key_row < start + WIN_ROWS)
                part = turned[:, skipped + j * tokens : skipped + (j + 1) * tokens]
                place = jnp.where(block % 2 == 0, j, blocks - 1 - j)
                bias_ref[place, head, lanes(r, GRID_W)] = jnp.where(inside, part, LOWEST)


def first_query(
    last_row, scaled_ref, scaler_ref, flat_ref, wq_hbm, wk_hbm, wv_hbm, wo_hbm, post_hbm,
    q_ref, bias_ref, wk_ref, wv_ref, wo_ref, post_ref, wq_ref, sems,
):
    copies = copying(
        (
            (wq_hbm.at[0], wq_ref),
            (wo_hbm.at[0], wo_ref),
            (post_hbm, post_ref),
            (wk_hbm.at[1], wk_ref),
            (wv_hbm.at[1], wv_ref),
        ),
        sems,
    )
    biases(last_row, lax.axis_index("sp"), flat_ref.at[0], bias_ref)
    copies[0].wait()
    q_ref[...] = query_from(scaled_ref, scaler_ref, wq_ref[...])
    for copy in copies[1:]:
        copy.wait()


def next_query(
    last_row, scaled_ref, scaler_ref, flat_ref, wq_hbm, wo_hbm,
    q_ref, bias_ref, wo_ref, wq_ref, sems,
):
    copies = copying(((wq_hbm.at[1], wq_ref), (wo_hbm.at[1], wo_ref)), sems)
    biases(last_row, lax.axis_index("sp"), flat_ref.at[1], bias_ref)
    copies[0].wait()
    q_ref[...] = query_from(scaled_ref, scaler_ref, wq_ref[...])
    copies[1].wait()


def next_heads(
    x_ref, b_ref, gain_ref, post_ref, wk_ref, wv_ref, kv_ref, scaled_ref, scaler_ref, own_ref
):
    count, tokens, feat = x_ref.shape
    squares = jnp.zeros((tokens, feat), jnp.float32)
    for i in range(count):
        branch = b_ref[i, :tokens].astype(jnp.float32)
        squares += branch * branch
    scale = scaler_of(squares, count * feat)
    squares = jnp.zeros((tokens, feat), jnp.float32)
    for i in range(count):
        parts = b_ref[i, tokens:].astype(jnp.float32)
        post = parts[0:1] + parts[1:2] + parts[2:3]
        branch = b_ref[i, :tokens].astype(jnp.float32)
        stream = (x_ref[i].astype(jnp.float32) + branch * scale * post).astype(jnp.bfloat16)
        wide = stream.astype(jnp.float32)
        squares += wide * wide
        scaled_ref[:, lanes(i, feat)] = (wide * gain_ref[1:2, lanes(i, feat)]).astype(jnp.bfloat16)
    scaler = scaler_of(squares, count * feat)
    scaler_ref[...] = scaler
    at = lax.axis_index("tp")
    own = x_ref[at].astype(jnp.float32)
    own_branch = b_ref[at][:tokens].astype(jnp.float32)
    own_ref[...] = (own + own_branch * scale * post_ref[0:1]).astype(jnp.bfloat16)
    key_value(scaled_ref[...], scaler, wk_ref[...], wv_ref[...], kv_ref)


def attend(q_ref, own_ref, cross_ref, within_ref, dc_ref, do_ref, dw_ref, bias_ref, out_ref):
    tokens, cols = q_ref.shape
    heads = cols // HEAD_DIM
    blocks = (cross_ref, own_ref, within_ref)
    key = jnp.concatenate([b[:tokens, :cols] for b in blocks], axis=0)
    value = jnp.concatenate([b[:tokens, cols:] for b in blocks], axis=0)
    key_docs = jnp.concatenate(
        [d[:1, :tokens].astype(jnp.float32) for d in (dc_ref, do_ref, dw_ref)], axis=1
    )
    query_docs = as_column(do_ref[:1, :tokens].astype(jnp.float32), tokens)
    same = key_docs == jnp.concatenate([query_docs] * 3, axis=1)
    query = q_ref[...]
    lane = lax.broadcasted_iota(jnp.int32, (tokens, cols), 1)
    split = jnp.concatenate(
        [jnp.where(lane // HEAD_DIM == h, query, jnp.zeros_like(query)) for h in range(heads)], axis=0
    )
    products = lax.dot_general(
        split, key, (((1,), (1,)), ((), ())), preferred_element_type=jnp.float32
    )
    bias = [jnp.concatenate([bias_ref[j, h] for j in range(len(blocks))], axis=1) for h in range(heads)]
    lifted = []
    for h in range(heads):
        scores = products[lanes(h, tokens)] * HEAD_DIM ** (-0.5) + bias[h]
        scores = jnp.where(same, scores, LOWEST)
        lifted.append(jnp.exp(scores - jnp.max(scores, axis=1, keepdims=True)))
    lifted = jnp.concatenate(lifted, axis=0)
    summed = jnp.dot(lifted.astype(jnp.bfloat16), value, preferred_element_type=jnp.float32)
    summed = summed / jnp.sum(lifted, axis=1, keepdims=True)
    result = summed[:tokens]
    for h in range(1, heads):
        result = jnp.where(lane // HEAD_DIM == h, summed[lanes(h, tokens)], result)
    out_ref[...] = jnp.broadcast_to(result.astype(jnp.bfloat16)[None], out_ref.shape)


def projected(a_ref, w_ref):
    joined = jnp.concatenate([a_ref[place(i, a_ref.shape[0])] for i in range(a_ref.shape[0])], axis=1)
    return jnp.dot(joined, w_ref[...], preferred_element_type=jnp.float32)


def first_out(a_ref, w_ref, post_ref, out_ref):
    tokens = a_ref.shape[1]
    out_ref[:tokens] = projected(a_ref, w_ref).astype(jnp.bfloat16)
    post = post_ref[0:1]
    high = post.astype(jnp.bfloat16).astype(jnp.float32)
    middle = (post - high).astype(jnp.bfloat16).astype(jnp.float32)
    low = post - high - middle
    place = lax.broadcasted_iota(jnp.int32, (out_ref.shape[0] - tokens, post.shape[1]), 0)
    rows = jnp.where(place == 0, high, jnp.where(place == 1, middle, low))
    out_ref[tokens:] = rows.astype(jnp.bfloat16)


def last_out(a_ref, w_ref, branch_ref, squares_ref):
    branch = projected(a_ref, w_ref)
    branch_ref[...] = branch
    squares = jnp.sum(jnp.transpose(branch * branch), axis=0, keepdims=True)
    squares_ref[...] = jnp.broadcast_to(squares[None], squares_ref.shape)


def finish(model_width, squares_ref, branch_ref, own_ref, post_ref, out_ref):
    total = jnp.sum(squares_ref[...], axis=0)
    scale = as_column(lax.rsqrt(total / model_width + EPSILON), branch_ref.shape[0])
    out_ref[...] = (
        own_ref[...].astype(jnp.float32) + branch_ref[...] * scale * post_ref[1:2]
    ).astype(jnp.bfloat16)


def neighbours(block):
    count = lax.axis_size("sp")
    edges = [[(i, i + 1), (i + 1, i)] for i in range(count - 1)]
    crossing = [pair for edge in edges[1::2] for pair in edge]
    within = [pair for edge in edges[0::2] for pair in edge]
    return lax.ppermute(block, "sp", crossing), lax.ppermute(block, "sp", within)


def gathered(block):
    return lax.all_gather(block, "tp", axis=0)


def place(index, count):
    return index % 2 * (count // 2) + index // 2


def gathered_by_core(copies):
    chips = copies.shape[0]
    across = [[core + 2 * chip for chip in range(chips)] for core in range(2)]
    pairs = [[2 * chip, 2 * chip + 1] for chip in range(chips)]
    same = lax.all_to_all(copies, "tp", 0, 0, axis_index_groups=across, tiled=True)
    both = lax.all_gather(same, "tp", axis=0, axis_index_groups=pairs)
    return both.reshape(2 * chips, *copies.shape[1:])


def shards(
    grid_in,
    documents,
    pre_gain,
    query_weight,
    key_weight,
    value_weight,
    offset_bias,
    out_weight,
    post_gain,
):
    tokens, feat = grid_in.shape
    _, model_width, cols = query_weight.shape
    heads = offset_bias.shape[1]
    bf16, f32 = jnp.bfloat16, jnp.float32
    members = lax.axis_size("tp")
    all_rows = tokens // GRID_W * lax.axis_size("sp")
    flat = jnp.pad(
        offset_bias, ((0, 0), (0, 0), (0, BIAS_ROWS - 2 * WIN_ROWS + 1), (0, GRID_W - 2 * WIN_COLS + 1))
    ).reshape(LAYERS, heads, BIAS_ROWS * GRID_W)
    weight = pltpu.VMEM((model_width, cols), bf16)
    shared = (pltpu.VMEM((tokens, model_width), bf16), pltpu.VMEM((tokens, feat), f32))

    stream = gathered(grid_in)
    kv, scaled, scaler, gain = call(
        first_heads,
        (pltpu.VMEM((tokens + PAD, 2 * cols), bf16), *shared, pltpu.VMEM(pre_gain.shape, f32)),
        [VMEM] + [HBM] * 4,
        "first_heads",
        [pltpu.VMEM((1, tokens), jnp.int32), weight, weight, pltpu.SemaphoreType.DMA((2 + 2 * CHUNKS,))],
    )(stream, pre_gain, documents.reshape(1, tokens), key_weight, value_weight)
    cross, within = neighbours(kv)
    bias_of = pltpu.VMEM((3, heads, tokens, tokens), f32)
    query, bias, wk, wv, out, post = call(
        functools.partial(first_query, all_rows),
        (
            pltpu.VMEM((tokens, cols), bf16),
            bias_of,
            *[weight] * 3,
            pltpu.VMEM(post_gain.shape, f32),
        ),
        [VMEM] * 3 + [HBM] * 5,
        "first_query",
        [weight, pltpu.SemaphoreType.DMA((5,))],
    )(scaled, scaler, flat, query_weight, key_weight, value_weight, out_weight, post_gain)
    doc_rows = (cross[tokens:], kv[tokens:], within[tokens:])

    def attention(query, kv, cross, within, bias):
        return call(attend, pltpu.VMEM((members // 2, tokens, cols), bf16), [VMEM] * 8, "attend")(
            query, kv, cross, within, *doc_rows, bias
        )

    attended = gathered_by_core(attention(query, kv, cross, within, bias))
    branch = call(first_out, pltpu.VMEM((tokens + PAD, feat), bf16), [VMEM] * 3, "first_out")(
        attended, out, post
    )
    branch = gathered(branch)
    kv, scaled, scaler, own = call(
        next_heads,
        (pltpu.VMEM((tokens, 2 * cols), bf16), *shared, pltpu.VMEM((tokens, feat), bf16)),
        [VMEM] * 6,
        "next_heads",
    )(stream, branch, gain, post, wk, wv)
    cross, within = neighbours(kv)
    query, bias, out = call(
        functools.partial(next_query, all_rows),
        (pltpu.VMEM((tokens, cols), bf16), bias_of, weight),
        [VMEM] * 3 + [HBM] * 2,
        "next_query",
        [weight, pltpu.SemaphoreType.DMA((2,))],
    )(scaled, scaler, flat, query_weight, out_weight)
    attended = gathered_by_core(attention(query, kv, cross, within, bias))
    branch, squares = call(
        last_out,
        (pltpu.VMEM((tokens, feat), f32), pltpu.VMEM((members, 1, tokens), f32)),
        [VMEM] * 2,
        "last_out",
    )(attended, out)
    squares = lax.all_to_all(squares, "tp", 0, 0, tiled=True)
    return call(
        functools.partial(finish, model_width),
        jax.ShapeDtypeStruct((tokens, feat), bf16),
        [VMEM] * 4,
        "finish",
    )(squares, branch, own, post)


def solution(mesh):
    return jax.shard_map(
        shards,
        mesh=mesh,
        in_specs=(
            P("sp", "tp"),
            P("sp"),
            P(),
            P(None, None, "tp"),
            P(None, None, "tp"),
            P(None, None, "tp"),
            P(None, "tp", None, None),
            P(None, None, "tp"),
            P(None, "tp"),
        ),
        out_specs=P("sp", "tp"),
        check_vma=False,
    )
```
